32 devices in a mesh: grp: 2 (over x), sp: 4 (over y, core), tp: 4 (over z).
Axes of the slice: x: 2, y: 2, z: 4, core: 2. Of those that a mesh axis runs over, the one named last changes fastest.
Arguments:
- stream: bfloat16 [2048, 2048], P(('grp', 'sp'), 'tp'), parts along dimension 0, may hold values from -6 to 6
- documents: int32 [2048], P(('grp', 'sp')), parts along dimension 0, may hold values from 0 to 1, never falling along the last dimension, each value on 1 to 768 neighbouring positions
- q_weight: bfloat16 [2, 2048, 2048], P(None, 'sp', 'tp'), may hold values from -0.125 to 0.125
- k_weight: bfloat16 [2, 2048, 2048], P(None, 'sp', 'tp'), may hold values from -0.125 to 0.125
- v_weight: bfloat16 [2, 2048, 2048], P(None, 'sp', 'tp'), may hold values from -0.125 to 0.125
- out_weight: bfloat16 [2, 2048, 2048], P(None, 'sp', 'tp'), may hold values from -0.125 to 0.125
- pre_gain: float32 [2, 2048], replicated, may hold values from 0.1 to 1.9
- post_gain: float32 [2, 2048], P(None, 'tp'), may hold values from 0.1 to 1.9
- offset_bias: float32 [2, 32, 15, 31], P(None, 'tp'), may hold values from -3 to 263
Outputs:
- result_stream: bfloat16 [2048, 2048], P(('grp', 'sp'), 'tp'), parts along dimension 0
The draws below stay inside these ranges and needn't reach their ends.
There are 2 independent parts, one for each index of `grp`. The reference program is written for one: setup_inputs(seed, part) draws one part's arguments, and reference() takes and returns one part's arrays. A program takes and returns all parts, laid end to end along the dimension named above; an argument that names none is the same for every part. Nothing has to cross between parts.
All inputs are finite; a program needn't handle non-finite values.
Results may differ from the reference program's by a relative error of at most 0.02.
Values may be sent and summed in bfloat16 or wider, within the bound.
A program may use at most 128 MiB of HBM per device.

```python
import math
import jax
import jax.numpy as jnp
import numpy as np
from jax import lax

HEADS = 32
HEAD_DIM = 64
D = 2048
GRID_W = 64
NA_ROWS = 8
NA_COLS = 16
LAYERS = 2
TOK_DEV = 256
TOKENS = 1024
N_SP = 4
N_TP = 4


def draw_offset_bias(key, part):
    table_shape = (LAYERS, HEADS, 2 * NA_ROWS - 1, 2 * NA_COLS - 1)
    base_bias = jnp.clip(0.5 * jax.random.normal(jax.random.fold_in(key, 11), table_shape, jnp.float32), -3.0, 3.0)
    return base_bias


def block_scale(rng, dims, shards, low, high):
    def one(position, shards_of):
        draws = jax.random.uniform(jax.random.fold_in(jax.random.fold_in(rng, 6), position), (shards_of,), jnp.float32, low / len(shards), high / len(shards))
        return jnp.repeat(jnp.exp(draws), dims[position] // shards_of).reshape((-1,) + (1,) * (len(dims) - position - 1))

    loudness = one(*shards[0])
    for cut in shards[1:]:
        loudness = loudness * one(*cut)
    return loudness


def split_up(amount, total, most, skew):
    portions = [(1 << 20) // math.isqrt(rank ** skew) + 1 for rank in range(2, amount + 1)]
    rest, given = total - most - (amount - 1), [1] * (amount - 1)
    while rest > 0:
        movable = [i for i in range(amount - 1) if given[i] < most]
        pool, remaining = sum([portions[i] for i in movable]), rest
        for i in movable:
            more = min(most - given[i], max(1, remaining * portions[i] // pool), rest)
            given[i] = given[i] + more
            rest = rest - more
    return np.array([most] + given)


def ragged(stream_key, amount, total, bound, skew):
    if amount == 2:
        one = jax.random.randint(stream_key, (), max(1, total - bound), min(bound, total - 1) + 1)
        return jnp.stack([one, total - one])
    sizes = jnp.asarray(split_up(amount, total, bound, skew), jnp.int32)
    couples = (amount - 1) // 2
    source_of, taker = sizes[1:1 + 2 * couples:2], sizes[2:2 + 2 * couples:2]
    slack = jnp.minimum(source_of - 1, bound - taker)
    moved = jax.random.randint(jax.random.fold_in(stream_key, 1), (couples,), 0, 1 << 20) % (slack + 1)
    sizes = sizes.at[1:1 + 2 * couples:2].set(source_of - moved).at[2:2 + 2 * couples:2].set(taker + moved)
    return sizes[jax.random.permutation(jax.random.fold_in(stream_key, 2), amount)]


def scatter_about(own_key, extent, width, bound, split=(), kind=jnp.bfloat16):
    drawn = jax.random.normal(own_key, extent, jnp.float32) * width
    if len(split) > 0:
        drawn = block_scale(own_key, extent, split, -0.22, 0.18) * drawn
    return jnp.clip(drawn, min=-bound, max=bound).astype(kind)


def setup_inputs(seed: int = 0, part: int = 0) -> dict:
    splits = jax.random.split(jax.random.key(seed), 10)
    own_keys = jax.random.split(jax.random.fold_in(splits[9], part), 10)
    stream = scatter_about(own_keys[0], (TOKENS, D), 1.0, 6.0, ((0, 4), (1, 4)))
    documents = jnp.searchsorted(jnp.cumsum(ragged(own_keys[1], max(2, N_SP // 2), TOKENS, 3 * TOK_DEV, 0)), jnp.arange(TOKENS), side="right").astype(jnp.int32)
    q_weight = scatter_about(splits[2], (LAYERS, D, D), D ** -0.5, 0.125, ((1, 4), (2, 4)))
    k_weight = scatter_about(splits[3], (LAYERS, D, D), D ** -0.5, 0.125, ((1, 4), (2, 4)))
    v_weight = scatter_about(splits[4], (LAYERS, D, D), D ** -0.5, 0.125, ((1, 4), (2, 4)))
    out_weight = scatter_about(splits[5], (LAYERS, D, D), D ** -0.5, 0.125, ((1, 4), (2, 4)))
    pre_gain = jnp.clip(1.0 + 0.18 * jax.random.normal(splits[6], (LAYERS, D), jnp.float32), 0.1, 1.9)
    post_gain = jnp.clip(1.0 + 0.18 * jax.random.normal(splits[7], (LAYERS, D), jnp.float32), 0.1, 1.9)
    offset_bias = draw_offset_bias(jax.random.fold_in(splits[9], 71), part)
    return dict(stream=stream, documents=documents, q_weight=q_weight, k_weight=k_weight, v_weight=v_weight, out_weight=out_weight, pre_gain=pre_gain, post_gain=post_gain, offset_bias=offset_bias)


EPS = 1e-06

def window_attention(queries, key_grid, value_grid, doc_grid, bias_table):
    total_rows = queries.shape[0]
    column_ids = jnp.arange(GRID_W).astype(jnp.int32)
    column_first = jnp.clip(column_ids - NA_COLS // 2, 0, GRID_W - NA_COLS)
    column_fits = (column_ids[None, :] >= column_first[:, None]) & (column_ids[None, :] < column_first[:, None] + NA_COLS)
    column_index = jnp.clip(column_ids[None, :] - column_ids[:, None] + NA_COLS - 1, 0, 2 * NA_COLS - 2)
    column_bias = bias_table[:, :, column_index]
    score_scale = HEAD_DIM ** (-0.5)

    def one_row(grid_row):
        row_start = jnp.clip(grid_row - NA_ROWS // 2, 0, total_rows - NA_ROWS).astype(jnp.int32)
        key_rows = lax.dynamic_slice_in_dim(key_grid, row_start, NA_ROWS, 0).astype(jnp.float32)
        value_rows = lax.dynamic_slice_in_dim(value_grid, row_start, NA_ROWS, 0).astype(jnp.float32)
        key_docs = lax.dynamic_slice_in_dim(doc_grid, row_start, NA_ROWS, 0)
        query_row = lax.dynamic_index_in_dim(queries, grid_row, 0, keepdims=False).astype(jnp.float32)
        query_docs = lax.dynamic_index_in_dim(doc_grid, grid_row, 0, keepdims=False)
        row_index = (row_start + jnp.arange(NA_ROWS).astype(jnp.int32) - grid_row + NA_ROWS - 1).astype(jnp.int32)
        row_bias = jnp.take(column_bias, row_index, axis=1).transpose(0, 2, 1, 3)
        scores = jnp.einsum('qhd,ikhd->hqik', query_row, key_rows) * score_scale + row_bias
        allowed = column_fits[:, None, :] & (key_docs[None, :, :] == query_docs[:, None, None])
        scores = jnp.where(allowed[None], scores, -jnp.inf)
        row_top = lax.optimization_barrier(jnp.max(scores, axis=(2, 3), keepdims=True))
        shifted_exp = jnp.exp(scores - row_top)
        weights = (shifted_exp / lax.optimization_barrier(jnp.sum(shifted_exp, axis=(2, 3), keepdims=True))).astype(jnp.bfloat16)
        return jnp.einsum('hqik,ikhd->qhd', weights.astype(jnp.float32), value_rows).astype(jnp.bfloat16)
    return lax.map(one_row, jnp.arange(total_rows).astype(jnp.int32))

def reference(stream, documents, q_weight, k_weight, v_weight, out_weight, pre_gain, post_gain, offset_bias):
    total_rows = TOKENS // GRID_W
    doc_grid = documents.reshape(total_rows, GRID_W)
    group_width = D // N_TP
    current = stream
    for layer_index in range(LAYERS):
        stream_f32 = current.astype(jnp.float32)
        inverse = lax.rsqrt(lax.optimization_barrier(jnp.mean(stream_f32 * stream_f32, axis=-1, keepdims=True)) + EPS)
        scaled = (stream_f32 * pre_gain[layer_index]).astype(jnp.bfloat16)

        def project(weight):
            product = jnp.dot(scaled, weight, preferred_element_type=jnp.float32) * inverse
            return product.astype(jnp.bfloat16).reshape(total_rows, GRID_W, HEADS, HEAD_DIM)
        attended = window_attention(project(q_weight[layer_index]), project(k_weight[layer_index]), project(v_weight[layer_index]), doc_grid, offset_bias[layer_index])
        attended = attended.reshape(TOKENS, D)
        branch = jnp.zeros((TOKENS, D), jnp.float32)
        for group_index in range(N_TP):
            lower = group_index * group_width
            upper = lower + group_width
            partial_value = jnp.dot(attended[:, lower:upper], out_weight[layer_index][:, lower:upper].T, preferred_element_type=jnp.float32)
            rounded = lax.optimization_barrier(partial_value.astype(jnp.bfloat16))
            branch = branch + rounded.astype(jnp.float32)
        out_inverse = lax.rsqrt(lax.optimization_barrier(jnp.mean(branch * branch, axis=-1, keepdims=True)) + EPS)
        current = (stream_f32 + branch * out_inverse * post_gain[layer_index]).astype(jnp.bfloat16)
    return current
```

```python
import functools

import jax
import jax.numpy as jnp
from jax import lax
from jax.experimental import pallas as pl
from jax.experimental.pallas import tpu as pltpu
from jax.sharding import PartitionSpec as P

HEAD_DIM = 64
GRID_W = 64
NA_ROWS = 8
NA_COLS = 16
HALF = NA_ROWS // 2
HALO = HALF * GRID_W
EPS = 1e-06
MESH = pl.DeviceIdType.MESH
F32 = jnp.float32
BF16 = jnp.bfloat16


def kernel(
    n_sp, n_tp, layers, tokens,
    x_ref, docq_ref, dock_ref, wq_ref, wk_ref, wv_ref, wo_ref, pre_ref, post_ref, tab_ref,
    out_ref,
    w_full, x_full, x_scaled, q_buf, k_ext, v_ext, d_ext, att, part, rs_buf, res, sq_own, sq_buf,
    bias, dmask,
    wl_sem, wy_send, wy_recv, wm_send, wm_recv, wf_send, wf_recv,
    xl_sem, x_send, x_recv, d_local, d_send, d_recv, h_send, h_recv, r_send, r_recv, s_send, s_recv,
):
    weights = (wq_ref, wk_ref, wv_ref, wo_ref)
    sp, tp = lax.axis_index("sp"), lax.axis_index("tp")
    n_y = n_sp // 2
    y, core = sp // 2, sp % 2
    mate = y * 2 + (1 - core)
    feats = x_ref.shape[1]
    width = wq_ref.shape[2]
    rows_w = wq_ref.shape[1]
    rows_dev = tokens // GRID_W
    n_pair = width // 128
    d_model = n_tp * feats

    def tp_at(shift):
        return (tp + shift) % n_tp

    def rows_of(owner):
        return pl.ds(pl.multiple_of(owner * rows_w, rows_w), rows_w)

    def remote(src, dst, send, recv, target):
        return pltpu.make_async_remote_copy(
            src_ref=src, dst_ref=dst, send_sem=send, recv_sem=recv,
            device_id=target, device_id_type=MESH,
        )

    barrier = pltpu.get_barrier_semaphore()
    for shift in range(1, n_tp):
        pl.semaphore_signal(barrier, inc=1, device_id={"tp": tp_at(shift)}, device_id_type=MESH)
    for shift in range(1, n_sp):
        pl.semaphore_signal(
            barrier, inc=1, device_id={"sp": (sp + shift) % n_sp}, device_id_type=MESH
        )
    pl.semaphore_wait(barrier, n_tp + n_sp - 2)

    def y_copy(slot, shift):
        mine = w_full.at[slot, rows_of(sp)]
        return remote(
            weights[slot % 4].at[slot // 4], mine, wy_send.at[slot, shift], wy_recv.at[slot, shift],
            {"sp": ((y + shift) % n_y) * 2 + core},
        )

    def mate_copy(slot):
        return remote(
            weights[slot % 4].at[slot // 4], w_full.at[slot, rows_of(sp)],
            wm_send.at[slot], wm_recv.at[slot], {"sp": mate},
        )

    def local_copy(slot):
        return pltpu.make_async_copy(
            weights[slot % 4].at[slot // 4], w_full.at[slot, rows_of(sp)], wl_sem.at[slot]
        )

    def forward_copy(slot, shift):
        block = w_full.at[slot, rows_of(((y - shift + n_y) % n_y) * 2 + core)]
        return remote(
            block, block, wf_send.at[slot, shift], wf_recv.at[slot, shift], {"sp": mate}
        )

    def start_weight(slot):
        for shift in range(1, n_y):
            y_copy(slot, shift).start()
        mate_copy(slot).start()
        local_copy(slot).start()

    def forward_weight(slot):
        for shift in range(1, n_y):
            y_copy(slot, shift).wait_recv()
            forward_copy(slot, shift).start()

    def finish_weight(slot):
        local_copy(slot).wait()
        mate_copy(slot).wait_recv()
        for shift in range(1, n_y):
            forward_copy(slot, shift).wait_recv()

    def drain_weight(slot):
        mate_copy(slot).wait_send()
        for shift in range(1, n_y):
            y_copy(slot, shift).wait_send()
            forward_copy(slot, shift).wait_send()

    def x_copy(layer, shift, source):
        return remote(
            source, x_full.at[layer, tp], x_send.at[layer, shift], x_recv.at[layer, shift],
            {"tp": tp_at(shift)},
        )

    def doc_copy(side):
        if side == 0:
            src, dst, target = dock_ref.at[pl.ds(rows_dev - HALF, HALF)], d_ext.at[pl.ds(0, HALF)], sp + 1
        else:
            src, dst, target = dock_ref.at[pl.ds(0, HALF)], d_ext.at[pl.ds(HALF + rows_dev, HALF)], sp - 1
        return remote(src, dst, d_send.at[side], d_recv.at[side], {"sp": target})

    def halo_copy(layer, side, which):
        buf = (k_ext, v_ext)[which]
        if side == 0:
            src, dst, target = tokens, 0, sp + 1
        else:
            src, dst, target = HALO, HALO + tokens, sp - 1
        return remote(
            buf.at[layer, pl.ds(src, HALO)], buf.at[layer, pl.ds(dst, HALO)],
            h_send.at[layer, side, which], h_recv.at[layer, side, which], {"sp": target},
        )

    has_next, has_prev = sp < n_sp - 1, sp > 0

    for slot in range(3):
        start_weight(slot)
    x_local = pltpu.make_async_copy(x_ref, x_full.at[0, tp], xl_sem)
    x_local.start()
    for shift in range(1, n_tp):
        x_copy(0, shift, x_ref).start()
    d_own = pltpu.make_async_copy(dock_ref, d_ext.at[pl.ds(HALF, rows_dev)], d_local)
    d_own.start()

    @pl.when(has_next)
    def _():
        doc_copy(0).start()

    @pl.when(has_prev)
    def _():
        doc_copy(1).start()

    q_ids = lax.broadcasted_iota(jnp.int32, (GRID_W, 128), 0)
    lanes = lax.broadcasted_iota(jnp.int32, (GRID_W, 128), 1)
    key_col = lanes % GRID_W
    first_col = jnp.clip(q_ids - NA_COLS // 2, 0, GRID_W - NA_COLS)
    col_ok = (key_col >= first_col) & (key_col < first_col + NA_COLS)
    low_half = lanes < GRID_W
    n_off = 2 * NA_ROWS - 2

    def expand(step, _):
        group, offset = step // n_off, step % n_off
        pair_rows = tab_ref[group, offset]
        for half in range(2):
            row = jnp.broadcast_to(pair_rows[half:half + 1], (GRID_W, 128))
            skew = pltpu.roll(row, 128 - (NA_COLS - 1), 1, stride=1, stride_axis=0)
            bias[group, offset, half * GRID_W:(half + 1) * GRID_W] = jnp.where(
                col_ok, skew, -jnp.inf
            )
        return 0

    lax.fori_loop(0, layers * n_pair * n_off, expand, 0)

    d_own.wait()

    @pl.when(has_next)
    def _():
        doc_copy(0).wait_send()
        doc_copy(1).wait_recv()

    @pl.when(has_prev)
    def _():
        doc_copy(1).wait_send()
        doc_copy(0).wait_recv()

    first_row = sp * rows_dev

    def window(row):
        start = jnp.clip(first_row + row - HALF, 0, rows_dev * n_sp - NA_ROWS)
        return start - first_row + HALF

    for row in range(rows_dev):
        q_doc = docq_ref[row * GRID_W:(row + 1) * GRID_W, :]
        for pair in range(NA_ROWS // 2):
            at = window(row) + 2 * pair
            k_doc = jnp.where(
                low_half,
                jnp.broadcast_to(d_ext[at][0:1], (GRID_W, 128)),
                jnp.broadcast_to(d_ext[at + 1][0:1], (GRID_W, 128)),
            )
            value = jnp.where(k_doc == q_doc, 0.0, -jnp.inf).astype(F32)
            dmask[row, pair, 0:GRID_W] = value
            dmask[row, pair, GRID_W:2 * GRID_W] = value

    x_local.wait()

    for layer in range(layers):
        base = 4 * layer
        for shift in range(1, n_tp):
            x_copy(layer, shift, x_ref).wait_recv()
        total = jnp.zeros((tokens, 1), F32)
        for block in range(n_tp):
            wide = x_full[layer, block].astype(F32)
            total = total + jnp.sum(wide * wide, axis=1, keepdims=True)
            gain = pre_ref[layer:layer + 1, block * feats:(block + 1) * feats]
            x_scaled[:, block * feats:(block + 1) * feats] = (wide * gain).astype(BF16)
        inverse = lax.rsqrt(total / d_model + EPS)

        for slot in range(base, base + 3):
            forward_weight(slot)
        for which in (1, 2, 0):
            finish_weight(base + which)
            product = jnp.dot(x_scaled[...], w_full[base + which], preferred_element_type=F32)
            rounded = (product * inverse).astype(BF16)
            if which == 0:
                q_buf[...] = rounded * jnp.asarray(HEAD_DIM ** -0.5, BF16)
            else:
                buf = (k_ext, v_ext)[which - 1]
                buf[layer, HALO:HALO + tokens] = rounded

                @pl.when(has_next)
                def _():
                    halo_copy(layer, 0, which - 1).start()

                @pl.when(has_prev)
                def _():
                    halo_copy(layer, 1, which - 1).start()

        start_weight(base + 3)
        if layer + 1 < layers:
            for slot in range(base + 4, base + 7):
                start_weight(slot)

        for which in range(2):
            @pl.when(has_next)
            def _():
                halo_copy(layer, 1, which).wait_recv()

            @pl.when(has_prev)
            def _():
                halo_copy(layer, 0, which).wait_recv()

        def attend(step, _):
            pair, row = step // rows_dev, step % rows_dev
            begin = window(row)
            cols = pl.ds(pl.multiple_of(pair * 128, 128), 128)
            q_rows = pl.ds(pl.multiple_of(row * GRID_W, GRID_W), GRID_W)
            keys = pl.ds(pl.multiple_of(begin * GRID_W, GRID_W), NA_ROWS * GRID_W)
            q2 = q_buf[q_rows, cols]
            zero = jnp.zeros_like(q2)
            stacked = jnp.concatenate(
                [jnp.where(low_half, q2, zero), jnp.where(low_half, zero, q2)], axis=0
            )
            k2 = k_ext[layer, keys, cols]
            scores = lax.dot_general(
                stacked, k2, (((1,), (1,)), ((), ())), preferred_element_type=F32
            )
            offset = begin - row + NA_ROWS - 1 - HALF
            pieces = []
            for at in range(NA_ROWS // 2):
                pieces.append(
                    scores[:, at * 128:(at + 1) * 128]
                    + bias[layer * n_pair + pair, offset + 2 * at]
                    + dmask[row, at]
                )
            full = jnp.concatenate(pieces, axis=1)
            top = jnp.max(full, axis=1, keepdims=True)
            grown = jnp.exp(full - top)
            share = 1.0 / jnp.sum(grown, axis=1, keepdims=True)
            probs = (grown * share).astype(BF16)
            mixed = jnp.dot(probs, v_ext[layer, keys, cols], preferred_element_type=F32)
            att[q_rows, cols] = jnp.where(low_half, mixed[:GRID_W], mixed[GRID_W:]).astype(BF16)
            return 0

        lax.fori_loop(0, n_pair * rows_dev, attend, 0)

        forward_weight(base + 3)
        finish_weight(base + 3)

        def r_copy(shift):
            return remote(
                part.at[layer, tp_at(shift)], rs_buf.at[layer, tp],
                r_send.at[layer, shift], r_recv.at[layer, shift], {"tp": tp_at(shift)},
            )

        for shift in list(range(1, n_tp)) + [0]:
            block = tp_at(shift)
            w_rows = pl.ds(pl.multiple_of(block * feats, feats), feats)
            product = lax.dot_general(
                att[...], w_full[base + 3, w_rows], (((1,), (1,)), ((), ())),
                preferred_element_type=F32,
            )
            part[layer, block] = product.astype(BF16)
            if shift:
                r_copy(shift).start()
        branch = part[layer, tp].astype(F32)
        for shift in range(1, n_tp):
            r_copy(shift).wait_recv()
            branch = branch + rs_buf[layer, tp_at(n_tp - shift)].astype(F32)
        squares = jnp.sum(branch * branch, axis=1, keepdims=True)
        flat = jnp.transpose(jnp.broadcast_to(squares, (tokens, 128)))
        sq_own[layer] = flat[0:8]

        def s_copy(shift):
            return remote(
                sq_own.at[layer], sq_buf.at[layer, tp],
                s_send.at[layer, shift], s_recv.at[layer, shift], {"tp": tp_at(shift)},
            )

        for shift in range(1, n_tp):
            s_copy(shift).start()
        summed = sq_own[layer]
        for shift in range(1, n_tp):
            s_copy(shift).wait_recv()
            summed = summed + sq_buf[layer, tp_at(n_tp - shift)]
        column = jnp.transpose(jnp.broadcast_to(summed[0:1], (128, tokens)))[:, 0:1]
        out_inverse = lax.rsqrt(column / d_model + EPS)
        before = x_ref[...] if layer == 0 else res[layer - 1]
        after = (
            before.astype(F32) + branch * out_inverse * post_ref[layer:layer + 1, :]
        ).astype(BF16)
        if layer + 1 < layers:
            res[layer] = after
            x_full[layer + 1, tp] = after
            for shift in range(1, n_tp):
                x_copy(layer + 1, shift, res.at[layer]).start()
        else:
            out_ref[...] = after
        for shift in range(1, n_tp):
            x_copy(layer, shift, x_ref).wait_send()
            r_copy(shift).wait_send()
            s_copy(shift).wait_send()
        for which in range(2):
            @pl.when(has_next)
            def _():
                halo_copy(layer, 0, which).wait_send()

            @pl.when(has_prev)
            def _():
                halo_copy(layer, 1, which).wait_send()
        for slot in range(base, base + 4):
            drain_weight(slot)


def shards(
    stream, documents, q_weight, k_weight, v_weight, out_weight, pre_gain, post_gain, offset_bias
):
    n_sp, n_tp = lax.axis_size("sp"), lax.axis_size("tp")
    tokens, feats = stream.shape
    layers, rows_w, width = q_weight.shape
    rows_dev = tokens // GRID_W
    n_pair = width // 128
    d_model = feats * n_tp
    n_off = 2 * NA_ROWS - 2
    doc_query = jnp.broadcast_to(documents[:, None], (tokens, 128))
    grid_docs = documents.reshape(rows_dev, 1, GRID_W)
    doc_key = jnp.broadcast_to(
        jnp.concatenate([grid_docs, grid_docs], axis=2), (rows_dev, 8, 2 * GRID_W)
    )
    table = jnp.pad(offset_bias, ((0, 0), (0, 0), (0, 0), (0, GRID_W - 2 * NA_COLS + 1)))
    table = jnp.concatenate([table[:, :, :-1], table[:, :, 1:]], axis=3)
    table = table.reshape(layers * n_pair, 2, n_off, 128).transpose(0, 2, 1, 3)
    n_y = n_sp // 2
    slots = 4 * layers
    ext = tokens + 2 * HALO
    dma = pltpu.SemaphoreType.DMA
    vmem = pl.BlockSpec(memory_space=pltpu.VMEM)
    hbm = pl.BlockSpec(memory_space=pl.ANY)
    return pl.pallas_call(
        functools.partial(kernel, n_sp, n_tp, layers, tokens),
        out_shape=jax.ShapeDtypeStruct((tokens, feats), BF16),
        in_specs=[vmem] * 3 + [hbm] * 4 + [vmem] * 3,
        out_specs=vmem,
        scratch_shapes=[
            pltpu.VMEM((slots, d_model, width), BF16),
            pltpu.VMEM((layers, n_tp, tokens, feats), BF16),
            pltpu.VMEM((tokens, d_model), BF16),
            pltpu.VMEM((tokens, width), BF16),
            pltpu.VMEM((layers, ext, width), BF16),
            pltpu.VMEM((layers, ext, width), BF16),
            pltpu.VMEM((rows_dev + 2 * HALF, 8, 128), jnp.int32),
            pltpu.VMEM((tokens, width), BF16),
            pltpu.VMEM((layers, n_tp, tokens, feats), BF16),
            pltpu.VMEM((layers, n_tp, tokens, feats), BF16),
            pltpu.VMEM((layers, tokens, feats), BF16),
            pltpu.VMEM((layers, 8, tokens), F32),
            pltpu.VMEM((layers, n_tp, 8, tokens), F32),
            pltpu.VMEM((layers * n_pair, n_off, 128, 128), F32),
            pltpu.VMEM((rows_dev, NA_ROWS // 2, 128, 128), F32),
            dma((slots,)),
            dma((slots, n_y)), dma((slots, n_y)),
            dma((slots,)), dma((slots,)),
            dma((slots, n_y)), dma((slots, n_y)),
            dma,
            dma((layers, n_tp)), dma((layers, n_tp)),
            dma, dma((2,)), dma((2,)),
            dma((layers, 2, 2)), dma((layers, 2, 2)),
            dma((layers, n_tp)), dma((layers, n_tp)),
            dma((layers, n_tp)), dma((layers, n_tp)),
        ],
        compiler_params=pltpu.CompilerParams(
            collective_id=0, has_side_effects=True, vmem_limit_bytes=60 * 1024 * 1024
        ),
    )(
        stream, doc_query, doc_key, q_weight, k_weight, v_weight, out_weight,
        pre_gain, post_gain, table,
    )


def solution(mesh):
    in_specs = (
        P(("grp", "sp"), "tp"),
        P(("grp", "sp")),
        P(None, "sp", "tp"),
        P(None, "sp", "tp"),
        P(None, "sp", "tp"),
        P(None, "sp", "tp"),
        P(),
        P(None, "tp"),
        P(None, "tp", None, None),
    )
    out_specs = P(("grp", "sp"), "tp")
    return jax.shard_map(shards, mesh=mesh, in_specs=in_specs, out_specs=out_specs, check_vma=False)
```

```python
import functools

import jax
import jax.numpy as jnp
from jax import lax
from jax.experimental import pallas as pl
from jax.experimental.pallas import tpu as pltpu
from jax.sharding import PartitionSpec as P

HEAD_DIM = 64
GRID_W = 64
NA_ROWS = 8
NA_COLS = 16
HALF = NA_ROWS // 2
HALO = HALF * GRID_W
EPS = 1e-06
MESH = pl.DeviceIdType.MESH
F32 = jnp.float32
BF16 = jnp.bfloat16


def kernel(
    n_sp, n_tp, n_grp, layers, tokens,
    x_ref, docq_ref, dock_ref, wq_ref, wk_ref, wv_ref, wo_ref, pre_ref, post_ref, tab_ref,
    out_ref,
    w_full, x_full, x_scaled, q_buf, k_ext, v_ext, d_ext, part, rs_buf, res, sq_own, sq_buf,
    bias, dmask,
    wl_sem, wy_send, wy_recv, wm_send, wm_recv, wf_send, wf_recv, wx_send, wx_recv,
    xl_sem, x_send, x_recv, d_local, d_send, d_recv, h_send, h_recv, r_send, r_recv, s_send, s_recv,
):
    weights = (wq_ref, wk_ref, wv_ref, wo_ref)
    sp, tp, grp = lax.axis_index("sp"), lax.axis_index("tp"), lax.axis_index("grp")
    n_y = n_sp // 2
    y, core = sp // 2, sp % 2
    mate = y * 2 + (1 - core)
    feats = x_ref.shape[1]
    width = wq_ref.shape[2]
    rows_w = wq_ref.shape[1]
    rows_dev = tokens // GRID_W
    n_pair = width // 128
    d_model = n_tp * feats

    def tp_at(shift):
        return (tp + shift) % n_tp

    piece = rows_w // n_grp

    def rows_of(owner):
        return pl.ds(pl.multiple_of(owner * rows_w, rows_w), rows_w)

    def piece_of(owner, index):
        return pl.ds(pl.multiple_of(owner * rows_w + index * piece, piece), piece)

    def remote(src, dst, send, recv, target):
        return pltpu.make_async_remote_copy(
            src_ref=src, dst_ref=dst, send_sem=send, recv_sem=recv,
            device_id=target, device_id_type=MESH,
        )

    barrier = pltpu.get_barrier_semaphore()
    for shift in range(1, n_tp):
        pl.semaphore_signal(barrier, inc=1, device_id={"tp": tp_at(shift)}, device_id_type=MESH)
    for shift in range(1, n_sp):
        pl.semaphore_signal(
            barrier, inc=1, device_id={"sp": (sp + shift) % n_sp}, device_id_type=MESH
        )
    for shift in range(1, n_grp):
        pl.semaphore_signal(
            barrier, inc=1, device_id={"grp": (grp + shift) % n_grp}, device_id_type=MESH
        )
    pl.semaphore_wait(barrier, n_tp + n_sp + n_grp - 3)

    def y_copy(slot, shift):
        own = pl.ds(pl.multiple_of(grp * piece, piece), piece)
        return remote(
            weights[slot % 4].at[slot // 4, own], w_full.at[slot, piece_of(sp, grp)],
            wy_send.at[slot, shift], wy_recv.at[slot, shift],
            {"sp": ((y + shift) % n_y) * 2 + core},
        )

    def mate_copy(slot):
        return remote(
            weights[slot % 4].at[slot // 4], w_full.at[slot, rows_of(sp)],
            wm_send.at[slot], wm_recv.at[slot], {"sp": mate},
        )

    def local_copy(slot):
        return pltpu.make_async_copy(
            weights[slot % 4].at[slot // 4], w_full.at[slot, rows_of(sp)], wl_sem.at[slot]
        )

    def arrived(slot, shift, turn):
        owner = ((y - shift + n_y) % n_y) * 2 + core
        return w_full.at[slot, piece_of(owner, (grp - turn + n_grp) % n_grp)]

    def forward_copy(slot, shift, turn):
        block = arrived(slot, shift, turn)
        return remote(
            block, block, wf_send.at[slot, shift, turn], wf_recv.at[slot, shift, turn],
            {"sp": mate},
        )

    def x_link_copy(slot, shift, turn):
        block = arrived(slot, shift, 0)
        return remote(
            block, block, wx_send.at[slot, shift, turn], wx_recv.at[slot, shift, turn],
            {"grp": (grp + turn) % n_grp},
        )

    def start_weight(slot):
        for shift in range(1, n_y):
            y_copy(slot, shift).start()
        mate_copy(slot).start()
        local_copy(slot).start()

    def pass_on(slot):
        for shift in range(1, n_y):
            y_copy(slot, shift).wait_recv()
            for turn in range(1, n_grp):
                x_link_copy(slot, shift, turn).start()
            forward_copy(slot, shift, 0).start()

    def pass_across(slot):
        for shift in range(1, n_y):
            for turn in range(1, n_grp):
                x_link_copy(slot, shift, turn).wait_recv()
                forward_copy(slot, shift, turn).start()

    def finish_weight(slot):
        local_copy(slot).wait()
        mate_copy(slot).wait_recv()
        for shift in range(1, n_y):
            for turn in range(n_grp):
                forward_copy(slot, shift, turn).wait_recv()

    def drain_weight(slot):
        mate_copy(slot).wait_send()
        for shift in range(1, n_y):
            y_copy(slot, shift).wait_send()
            for turn in range(n_grp):
                forward_copy(slot, shift, turn).wait_send()
            for turn in range(1, n_grp):
                x_link_copy(slot, shift, turn).wait_send()

    def x_copy(layer, shift, source):
        return remote(
            source, x_full.at[layer, tp], x_send.at[layer, shift], x_recv.at[layer, shift],
            {"tp": tp_at(shift)},
        )

    def doc_copy(side):
        if side == 0:
            src, dst, target = dock_ref.at[pl.ds(rows_dev - HALF, HALF)], d_ext.at[pl.ds(0, HALF)], sp + 1
        else:
            src, dst, target = dock_ref.at[pl.ds(0, HALF)], d_ext.at[pl.ds(HALF + rows_dev, HALF)], sp - 1
        return remote(src, dst, d_send.at[side], d_recv.at[side], {"sp": target})

    def halo_copy(layer, side, which):
        buf = (k_ext, v_ext)[which]
        if side == 0:
            src, dst, target = tokens, 0, sp + 1
        else:
            src, dst, target = HALO, HALO + tokens, sp - 1
        return remote(
            buf.at[layer, pl.ds(src, HALO)], buf.at[layer, pl.ds(dst, HALO)],
            h_send.at[layer, side, which], h_recv.at[layer, side, which], {"sp": target},
        )

    has_next, has_prev = sp < n_sp - 1, sp > 0

    order = (1, 2, 0, 3)
    for slot in order:
        start_weight(slot)
    x_local = pltpu.make_async_copy(x_ref, x_full.at[0, tp], xl_sem)
    x_local.start()
    for shift in range(1, n_tp):
        x_copy(0, shift, x_ref).start()
    d_own = pltpu.make_async_copy(dock_ref, d_ext.at[pl.ds(HALF, rows_dev)], d_local)
    d_own.start()

    @pl.when(has_next)
    def _():
        doc_copy(0).start()

    @pl.when(has_prev)
    def _():
        doc_copy(1).start()

    q_ids = lax.broadcasted_iota(jnp.int32, (GRID_W, 128), 0)
    lanes = lax.broadcasted_iota(jnp.int32, (GRID_W, 128), 1)
    key_col = lanes % GRID_W
    first_col = jnp.clip(q_ids - NA_COLS // 2, 0, GRID_W - NA_COLS)
    col_ok = (key_col >= first_col) & (key_col < first_col + NA_COLS)
    low_half = lanes < GRID_W
    n_off = 2 * NA_ROWS - 2

    def expand(step, _):
        group, offset = step // n_off, step % n_off
        pair_rows = tab_ref[group, offset]
        for half in range(2):
            row = jnp.broadcast_to(pair_rows[half:half + 1], (GRID_W, 128))
            skew = pltpu.roll(row, 128 - (NA_COLS - 1), 1, stride=1, stride_axis=0)
            bias[group, offset, half * GRID_W:(half + 1) * GRID_W] = jnp.where(
                col_ok, skew, -jnp.inf
            )
        return 0

    lax.fori_loop(0, layers * n_pair * n_off, expand, 0)

    d_own.wait()

    @pl.when(has_next)
    def _():
        doc_copy(0).wait_send()
        doc_copy(1).wait_recv()

    @pl.when(has_prev)
    def _():
        doc_copy(1).wait_send()
        doc_copy(0).wait_recv()

    first_row = sp * rows_dev

    def window(row):
        start = jnp.clip(first_row + row - HALF, 0, rows_dev * n_sp - NA_ROWS)
        return start - first_row + HALF

    for row in range(rows_dev):
        q_doc = docq_ref[row * GRID_W:(row + 1) * GRID_W, :]
        for pair in range(NA_ROWS // 2):
            at = window(row) + 2 * pair
            k_doc = jnp.where(
                low_half,
                jnp.broadcast_to(d_ext[at][0:1], (GRID_W, 128)),
                jnp.broadcast_to(d_ext[at + 1][0:1], (GRID_W, 128)),
            )
            value = jnp.where(k_doc == q_doc, 0.0, -jnp.inf).astype(F32)
            dmask[row, pair, 0:GRID_W] = value
            dmask[row, pair, GRID_W:2 * GRID_W] = value

    for slot in order[:3]:
        pass_on(slot)
    for slot in order[:2]:
        pass_across(slot)
    x_local.wait()

    for layer in range(layers):
        base = 4 * layer
        for shift in range(1, n_tp):
            x_copy(layer, shift, x_ref).wait_recv()
        total = jnp.zeros((tokens, 1), F32)
        for block in range(n_tp):
            wide = x_full[layer, block].astype(F32)
            total = total + jnp.sum(wide * wide, axis=1, keepdims=True)
            gain = pre_ref[layer:layer + 1, block * feats:(block + 1) * feats]
            x_scaled[:, block * feats:(block + 1) * feats] = (wide * gain).astype(BF16)
        inverse = lax.rsqrt(total / d_model + EPS)

        if layer == 0:
            pass_across(order[2])
        for which in order[:3]:
            finish_weight(base + which)
            product = jnp.dot(x_scaled[...], w_full[base + which], preferred_element_type=F32)
            rounded = (product * inverse).astype(BF16)
            if which == 0:
                q_buf[...] = rounded * jnp.asarray(HEAD_DIM ** -0.5, BF16)
            else:
                buf = (k_ext, v_ext)[which - 1]
                buf[layer, HALO:HALO + tokens] = rounded

                @pl.when(has_next)
                def _():
                    halo_copy(layer, 0, which - 1).start()

                @pl.when(has_prev)
                def _():
                    halo_copy(layer, 1, which - 1).start()

        if layer + 1 < layers:
            for slot in order:
                start_weight(base + 4 + slot)
        if layer == 0:
            pass_on(3)
            pass_across(3)

        for which in range(2):
            @pl.when(has_next)
            def _():
                halo_copy(layer, 1, which).wait_recv()

            @pl.when(has_prev)
            def _():
                halo_copy(layer, 0, which).wait_recv()

        finish_weight(base + 3)

        def r_copy(row, shift):
            here = pl.ds(pl.multiple_of(row * GRID_W, GRID_W), GRID_W)
            return remote(
                part.at[layer, tp_at(shift), here], rs_buf.at[layer, tp, here],
                r_send.at[layer, row, shift], r_recv.at[layer, row, shift],
                {"tp": tp_at(shift)},
            )

        def attend(row, _):
            begin = window(row)
            q_rows = pl.ds(pl.multiple_of(row * GRID_W, GRID_W), GRID_W)
            keys = pl.ds(pl.multiple_of(begin * GRID_W, GRID_W), NA_ROWS * GRID_W)
            offset = begin - row + NA_ROWS - 1 - HALF
            attended = []
            for pair in range(n_pair):
                cols = slice(pair * 128, (pair + 1) * 128)
                q2 = q_buf[q_rows, cols]
                zero = jnp.zeros_like(q2)
                stacked = jnp.concatenate(
                    [jnp.where(low_half, q2, zero), jnp.where(low_half, zero, q2)], axis=0
                )
                k2 = k_ext[layer, keys, cols]
                scores = lax.dot_general(
                    stacked, k2, (((1,), (1,)), ((), ())), preferred_element_type=F32
                )
                pieces = []
                for at in range(NA_ROWS // 2):
                    pieces.append(
                        scores[:, at * 128:(at + 1) * 128]
                        + bias[layer * n_pair + pair, offset + 2 * at]
                        + dmask[row, at]
                    )
                full = jnp.concatenate(pieces, axis=1)
                top = jnp.max(full, axis=1, keepdims=True)
                grown = jnp.exp(full - top)
                share = 1.0 / jnp.sum(grown, axis=1, keepdims=True)
                probs = (grown * share).astype(BF16)
                mixed = jnp.dot(probs, v_ext[layer, keys, cols], preferred_element_type=F32)
                attended.append(
                    jnp.where(low_half, mixed[:GRID_W], mixed[GRID_W:]).astype(BF16)
                )
            attended = jnp.concatenate(attended, axis=1)
            for shift in list(range(1, n_tp)) + [0]:
                block = tp_at(shift)
                w_rows = pl.ds(pl.multiple_of(block * feats, feats), feats)
                product = lax.dot_general(
                    attended, w_full[base + 3, w_rows], (((1,), (1,)), ((), ())),
                    preferred_element_type=F32,
                )
                part[layer, block, q_rows] = product.astype(BF16)
                if shift:
                    r_copy(row, shift).start()
            return 0

        lax.fori_loop(0, rows_dev, attend, 0)

        if layer + 1 < layers:
            for slot in order:
                pass_on(base + 4 + slot)
        branch = part[layer, tp].astype(F32)
        for shift in range(1, n_tp):
            for row in range(rows_dev):
                r_copy(row, shift).wait_recv()
            branch = branch + rs_buf[layer, tp_at(n_tp - shift)].astype(F32)
        squares = jnp.sum(branch * branch, axis=1, keepdims=True)
        flat = jnp.transpose(jnp.broadcast_to(squares, (tokens, 128)))
        sq_own[layer] = flat[0:8]

        def s_copy(shift):
            return remote(
                sq_own.at[layer], sq_buf.at[layer, tp],
                s_send.at[layer, shift], s_recv.at[layer, shift], {"tp": tp_at(shift)},
            )

        for shift in range(1, n_tp):
            s_copy(shift).start()
        summed = sq_own[layer]
        for shift in range(1, n_tp):
            s_copy(shift).wait_recv()
            summed = summed + sq_buf[layer, tp_at(n_tp - shift)]
        column = jnp.transpose(jnp.broadcast_to(summed[0:1], (128, tokens)))[:, 0:1]
        out_inverse = lax.rsqrt(column / d_model + EPS)
        before = x_ref[...] if layer == 0 else res[layer - 1]
        after = (
            before.astype(F32) + branch * out_inverse * post_ref[layer:layer + 1, :]
        ).astype(BF16)
        if layer + 1 < layers:
            res[layer] = after
            x_full[layer + 1, tp] = after
            for shift in range(1, n_tp):
                x_copy(layer + 1, shift, res.at[layer]).start()
            for slot in order:
                pass_across(base + 4 + slot)
        else:
            out_ref[...] = after
        for shift in range(1, n_tp):
            x_copy(layer, shift, x_ref).wait_send()
            for row in range(rows_dev):
                r_copy(row, shift).wait_send()
            s_copy(shift).wait_send()
        for which in range(2):
            @pl.when(has_next)
            def _():
                halo_copy(layer, 0, which).wait_send()

            @pl.when(has_prev)
            def _():
                halo_copy(layer, 1, which).wait_send()
        for slot in range(base, base + 4):
            drain_weight(slot)


def shards(
    stream, documents, q_weight, k_weight, v_weight, out_weight, pre_gain, post_gain, offset_bias
):
    n_sp, n_tp, n_grp = lax.axis_size("sp"), lax.axis_size("tp"), lax.axis_size("grp")
    tokens, feats = stream.shape
    layers, rows_w, width = q_weight.shape
    rows_dev = tokens // GRID_W
    n_pair = width // 128
    d_model = feats * n_tp
    n_off = 2 * NA_ROWS - 2
    doc_query = jnp.broadcast_to(documents[:, None], (tokens, 128))
    grid_docs = documents.reshape(rows_dev, 1, GRID_W)
    doc_key = jnp.broadcast_to(
        jnp.concatenate([grid_docs, grid_docs], axis=2), (rows_dev, 8, 2 * GRID_W)
    )
    table = jnp.pad(offset_bias, ((0, 0), (0, 0), (0, 0), (0, GRID_W - 2 * NA_COLS + 1)))
    table = jnp.concatenate([table[:, :, :-1], table[:, :, 1:]], axis=3)
    table = table.reshape(layers * n_pair, 2, n_off, 128).transpose(0, 2, 1, 3)
    n_y = n_sp // 2
    slots = 4 * layers
    ext = tokens + 2 * HALO
    dma = pltpu.SemaphoreType.DMA
    vmem = pl.BlockSpec(memory_space=pltpu.VMEM)
    hbm = pl.BlockSpec(memory_space=pl.ANY)
    return pl.pallas_call(
        functools.partial(kernel, n_sp, n_tp, n_grp, layers, tokens),
        out_shape=jax.ShapeDtypeStruct((tokens, feats), BF16),
        in_specs=[vmem] * 3 + [hbm] * 4 + [vmem] * 3,
        out_specs=vmem,
        scratch_shapes=[
            pltpu.VMEM((slots, d_model, width), BF16),
            pltpu.VMEM((layers, n_tp, tokens, feats), BF16),
            pltpu.VMEM((tokens, d_model), BF16),
            pltpu.VMEM((tokens, width), BF16),
            pltpu.VMEM((layers, ext, width), BF16),
            pltpu.VMEM((layers, ext, width), BF16),
            pltpu.VMEM((rows_dev + 2 * HALF, 8, 128), jnp.int32),
            pltpu.VMEM((layers, n_tp, tokens, feats), BF16),
            pltpu.VMEM((layers, n_tp, tokens, feats), BF16),
            pltpu.VMEM((layers, tokens, feats), BF16),
            pltpu.VMEM((layers, 8, tokens), F32),
            pltpu.VMEM((layers, n_tp, 8, tokens), F32),
            pltpu.VMEM((layers * n_pair, n_off, 128, 128), F32),
            pltpu.VMEM((rows_dev, NA_ROWS // 2, 128, 128), F32),
            dma((slots,)),
            dma((slots, n_y)), dma((slots, n_y)),
            dma((slots,)), dma((slots,)),
            dma((slots, n_y, n_grp)), dma((slots, n_y, n_grp)),
            dma((slots, n_y, n_grp)), dma((slots, n_y, n_grp)),
            dma,
            dma((layers, n_tp)), dma((layers, n_tp)),
            dma, dma((2,)), dma((2,)),
            dma((layers, 2, 2)), dma((layers, 2, 2)),
            dma((layers, rows_dev, n_tp)), dma((layers, rows_dev, n_tp)),
            dma((layers, n_tp)), dma((layers, n_tp)),
        ],
        compiler_params=pltpu.CompilerParams(
            collective_id=0, has_side_effects=True, vmem_limit_bytes=60 * 1024 * 1024
        ),
    )(
        stream, doc_query, doc_key, q_weight, k_weight, v_weight, out_weight,
        pre_gain, post_gain, table,
    )


def solution(mesh):
    in_specs = (
        P(("grp", "sp"), "tp"),
        P(("grp", "sp")),
        P(None, "sp", "tp"),
        P(None, "sp", "tp"),
        P(None, "sp", "tp"),
        P(None, "sp", "tp"),
        P(),
        P(None, "tp"),
        P(None, "tp", None, None),
    )
    out_specs = P(("grp", "sp"), "tp")
    return jax.shard_map(shards, mesh=mesh, in_specs=in_specs, out_specs=out_specs, check_vma=False)
```

```python
import functools

import jax
import jax.numpy as jnp
from jax import lax
from jax.experimental import pallas as pl
from jax.experimental.pallas import tpu as pltpu
from jax.sharding import PartitionSpec as P

HEAD_DIM = 64
GRID_W = 64
NA_ROWS = 8
NA_COLS = 16
HALF = NA_ROWS // 2
HALO = HALF * GRID_W
EPS = 1e-06
MESH = pl.DeviceIdType.MESH
F32 = jnp.float32
BF16 = jnp.bfloat16


def kernel(
    n_sp, n_tp, n_grp, layers, tokens,
    x_ref, dock_ref, wq_ref, wk_ref, wv_ref, wo_ref, pre_ref, post_ref, tab_ref,
    out_ref,
    w_full, x_full, x_scaled, q_buf, k_ext, v_ext, d_ext, part, rs_buf, res, sq_own, sq_buf,
    bias, dmask,
    wl_sem, wy_send, wy_recv, wm_send, wm_recv, wf_send, wf_recv, wx_send, wx_recv,
    xl_sem, x_send, x_recv, d_local, d_send, d_recv, h_send, h_recv, r_send, r_recv, s_send, s_recv,
):
    weights = (wq_ref, wk_ref, wv_ref, wo_ref)
    sp, tp, grp = lax.axis_index("sp"), lax.axis_index("tp"), lax.axis_index("grp")
    n_y = n_sp // 2
    y, core = sp // 2, sp % 2
    mate = y * 2 + (1 - core)
    feats = x_ref.shape[1]
    width = wq_ref.shape[2]
    rows_w = wq_ref.shape[1]
    rows_dev = tokens // GRID_W
    n_pair = width // 128
    d_model = n_tp * feats

    def tp_at(shift):
        return (tp + shift) % n_tp

    piece = rows_w // n_grp

    def rows_of(owner):
        return pl.ds(pl.multiple_of(owner * rows_w, rows_w), rows_w)

    def piece_of(owner, index):
        return pl.ds(pl.multiple_of(owner * rows_w + index * piece, piece), piece)

    def remote(src, dst, send, recv, target):
        return pltpu.make_async_remote_copy(
            src_ref=src, dst_ref=dst, send_sem=send, recv_sem=recv,
            device_id=target, device_id_type=MESH,
        )

    barrier = pltpu.get_barrier_semaphore()
    for shift in range(1, n_tp):
        pl.semaphore_signal(barrier, inc=1, device_id={"tp": tp_at(shift)}, device_id_type=MESH)
    for shift in range(1, n_sp):
        pl.semaphore_signal(
            barrier, inc=1, device_id={"sp": (sp + shift) % n_sp}, device_id_type=MESH
        )
    for shift in range(1, n_grp):
        pl.semaphore_signal(
            barrier, inc=1, device_id={"grp": (grp + shift) % n_grp}, device_id_type=MESH
        )
    pl.semaphore_wait(barrier, n_tp + n_sp + n_grp - 3)

    def y_copy(slot, shift):
        own = pl.ds(pl.multiple_of(grp * piece, piece), piece)
        return remote(
            weights[slot % 4].at[slot // 4, own], w_full.at[slot, piece_of(sp, grp)],
            wy_send.at[slot, shift], wy_recv.at[slot, shift],
            {"sp": ((y + shift) % n_y) * 2 + core},
        )

    def mate_copy(slot):
        return remote(
            weights[slot % 4].at[slot // 4], w_full.at[slot, rows_of(sp)],
            wm_send.at[slot], wm_recv.at[slot], {"sp": mate},
        )

    def local_copy(slot):
        return pltpu.make_async_copy(
            weights[slot % 4].at[slot // 4], w_full.at[slot, rows_of(sp)], wl_sem.at[slot]
        )

    def arrived(slot, shift, turn):
        owner = ((y - shift + n_y) % n_y) * 2 + core
        return w_full.at[slot, piece_of(owner, (grp - turn + n_grp) % n_grp)]

    def forward_copy(slot, shift, turn):
        block = arrived(slot, shift, turn)
        return remote(
            block, block, wf_send.at[slot, shift, turn], wf_recv.at[slot, shift, turn],
            {"sp": mate},
        )

    def x_link_copy(slot, shift, turn):
        block = arrived(slot, shift, 0)
        return remote(
            block, block, wx_send.at[slot, shift, turn], wx_recv.at[slot, shift, turn],
            {"grp": (grp + turn) % n_grp},
        )

    def start_weight(slot):
        for shift in range(1, n_y):
            y_copy(slot, shift).start()
        mate_copy(slot).start()
        local_copy(slot).start()

    def pass_on(slot):
        for shift in range(1, n_y):
            y_copy(slot, shift).wait_recv()
            for turn in range(1, n_grp):
                x_link_copy(slot, shift, turn).start()
            forward_copy(slot, shift, 0).start()

    def pass_across(slot):
        for shift in range(1, n_y):
            for turn in range(1, n_grp):
                x_link_copy(slot, shift, turn).wait_recv()
                forward_copy(slot, shift, turn).start()

    def finish_weight(slot):
        local_copy(slot).wait()
        mate_copy(slot).wait_recv()
        for shift in range(1, n_y):
            for turn in range(n_grp):
                forward_copy(slot, shift, turn).wait_recv()

    def drain_weight(slot):
        mate_copy(slot).wait_send()
        for shift in range(1, n_y):
            y_copy(slot, shift).wait_send()
            for turn in range(n_grp):
                forward_copy(slot, shift, turn).wait_send()
            for turn in range(1, n_grp):
                x_link_copy(slot, shift, turn).wait_send()

    def x_copy(layer, shift, source):
        return remote(
            source, x_full.at[layer, tp], x_send.at[layer, shift], x_recv.at[layer, shift],
            {"tp": tp_at(shift)},
        )

    def doc_copy(side):
        if side == 0:
            src, dst, target = dock_ref.at[pl.ds(rows_dev - HALF, HALF)], d_ext.at[pl.ds(0, HALF)], sp + 1
        else:
            src, dst, target = dock_ref.at[pl.ds(0, HALF)], d_ext.at[pl.ds(HALF + rows_dev, HALF)], sp - 1
        return remote(src, dst, d_send.at[side], d_recv.at[side], {"sp": target})

    def halo_copy(layer, side, which):
        buf = (k_ext, v_ext)[which]
        if side == 0:
            src, dst, target = tokens, 0, sp + 1
        else:
            src, dst, target = HALO, HALO + tokens, sp - 1
        return remote(
            buf.at[layer, pl.ds(src, HALO)], buf.at[layer, pl.ds(dst, HALO)],
            h_send.at[layer, side, which], h_recv.at[layer, side, which], {"sp": target},
        )

    has_next, has_prev = sp < n_sp - 1, sp > 0

    order = (1, 2, 0, 3)
    for slot in order:
        start_weight(slot)
    x_local = pltpu.make_async_copy(x_ref, x_full.at[0, tp], xl_sem)
    x_local.start()
    for shift in range(1, n_tp):
        x_copy(0, shift, x_ref).start()
    d_own = pltpu.make_async_copy(dock_ref, d_ext.at[pl.ds(HALF, rows_dev)], d_local)
    d_own.start()

    @pl.when(has_next)
    def _():
        doc_copy(0).start()

    @pl.when(has_prev)
    def _():
        doc_copy(1).start()

    q_ids = lax.broadcasted_iota(jnp.int32, (GRID_W, 128), 0)
    lanes = lax.broadcasted_iota(jnp.int32, (GRID_W, 128), 1)
    key_col = lanes % GRID_W
    first_col = jnp.clip(q_ids - NA_COLS // 2, 0, GRID_W - NA_COLS)
    col_ok = (key_col >= first_col) & (key_col < first_col + NA_COLS)
    low_half = lanes < GRID_W
    n_off = 2 * NA_ROWS - 2

    def expand(step, _):
        group, offset = step // n_off, step % n_off
        for half in range(2):
            first = tab_ref[group * 2 + half, pl.ds(offset, 1)]
            second = tab_ref[group * 2 + half, pl.ds(offset + 1, 1)]
            row = jnp.broadcast_to(first + pltpu.roll(second, GRID_W, 1), (GRID_W, 128))
            skew = pltpu.roll(row, 128 - (NA_COLS - 1), 1, stride=1, stride_axis=0)
            bias[group, offset, half * GRID_W:(half + 1) * GRID_W] = jnp.where(
                col_ok, skew, -jnp.inf
            )
        return 0

    def expand_layer(layer):
        lax.fori_loop(layer * n_pair * n_off, (layer + 1) * n_pair * n_off, expand, 0)

    expand_layer(0)
    pass_on(order[0])

    d_own.wait()

    @pl.when(has_next)
    def _():
        doc_copy(0).wait_send()
        doc_copy(1).wait_recv()

    @pl.when(has_prev)
    def _():
        doc_copy(1).wait_send()
        doc_copy(0).wait_recv()

    first_row = sp * rows_dev

    def window(row):
        start = jnp.clip(first_row + row - HALF, 0, rows_dev * n_sp - NA_ROWS)
        return start - first_row + HALF

    for row in range(rows_dev):
        own_docs = jnp.broadcast_to(dock_ref[row][0:1].astype(F32), (128, 128))
        q_doc = jnp.transpose(own_docs)[0:GRID_W]
        for pair in range(NA_ROWS // 2):
            at = window(row) + 2 * pair
            k_doc = jnp.where(
                low_half,
                jnp.broadcast_to(d_ext[at][0:1], (GRID_W, 128)),
                jnp.broadcast_to(d_ext[at + 1][0:1], (GRID_W, 128)),
            )
            value = jnp.where(k_doc.astype(F32) == q_doc, 0.0, -jnp.inf).astype(F32)
            dmask[row, pair, 0:GRID_W] = value
            dmask[row, pair, GRID_W:2 * GRID_W] = value

    pass_on(order[1])
    pass_across(order[0])
    x_local.wait()

    for layer in range(layers):
        base = 4 * layer
        total = jnp.zeros((tokens, 1), F32)
        for shift in range(n_tp):
            if shift:
                x_copy(layer, shift, x_ref).wait_recv()
            block = tp_at(n_tp - shift)
            span = pl.ds(pl.multiple_of(block * feats, feats), feats)
            wide = x_full[layer, block].astype(F32)
            total = total + jnp.sum(wide * wide, axis=1, keepdims=True)
            x_scaled[:, span] = (wide * pre_ref[layer:layer + 1, span]).astype(BF16)
            if layer == 0 and shift == min(1, n_tp - 1):
                pass_on(order[2])
                pass_across(order[1])
        inverse = lax.rsqrt(total / d_model + EPS)

        if layer == 0:
            pass_on(order[3])
            pass_across(order[2])
        for which in order[:3]:
            finish_weight(base + which)
            product = jnp.dot(x_scaled[...], w_full[base + which], preferred_element_type=F32)
            rounded = (product * inverse).astype(BF16)
            if which == 0:
                q_buf[...] = rounded * jnp.asarray(HEAD_DIM ** -0.5, BF16)
            else:
                buf = (k_ext, v_ext)[which - 1]
                buf[layer, HALO:HALO + tokens] = rounded

                @pl.when(has_next)
                def _():
                    halo_copy(layer, 0, which - 1).start()

                @pl.when(has_prev)
                def _():
                    halo_copy(layer, 1, which - 1).start()

        if layer + 1 < layers:
            for slot in order:
                start_weight(base + 4 + slot)
        if layer == 0:
            pass_across(order[3])

        for which in range(2):
            @pl.when(has_next)
            def _():
                halo_copy(layer, 1, which).wait_recv()

            @pl.when(has_prev)
            def _():
                halo_copy(layer, 0, which).wait_recv()

        finish_weight(base + 3)

        def r_copy(row, shift):
            here = pl.ds(pl.multiple_of(row * GRID_W, GRID_W), GRID_W)
            return remote(
                part.at[layer, tp_at(shift), here], rs_buf.at[layer, tp, here],
                r_send.at[layer, row, shift], r_recv.at[layer, row, shift],
                {"tp": tp_at(shift)},
            )

        def attend(row, _):
            begin = window(row)
            q_rows = pl.ds(pl.multiple_of(row * GRID_W, GRID_W), GRID_W)
            keys = pl.ds(pl.multiple_of(begin * GRID_W, GRID_W), NA_ROWS * GRID_W)
            offset = begin - row + NA_ROWS - 1 - HALF
            attended = []
            for pair in range(n_pair):
                cols = slice(pair * 128, (pair + 1) * 128)
                q2 = q_buf[q_rows, cols]
                zero = jnp.zeros_like(q2)
                stacked = jnp.concatenate(
                    [jnp.where(low_half, q2, zero), jnp.where(low_half, zero, q2)], axis=0
                )
                k2 = k_ext[layer, keys, cols]
                scores = lax.dot_general(
                    stacked, k2, (((1,), (1,)), ((), ())), preferred_element_type=F32
                )
                pieces = []
                for at in range(NA_ROWS // 2):
                    pieces.append(
                        scores[:, at * 128:(at + 1) * 128]
                        + bias[layer * n_pair + pair, offset + 2 * at]
                        + dmask[row, at]
                    )
                full = jnp.concatenate(pieces, axis=1)
                top = jnp.max(full, axis=1, keepdims=True)
                grown = jnp.exp(full - top)
                share = 1.0 / jnp.sum(grown, axis=1, keepdims=True)
                probs = (grown * share).astype(BF16)
                mixed = jnp.dot(probs, v_ext[layer, keys, cols], preferred_element_type=F32)
                attended.append(
                    jnp.where(low_half, mixed[:GRID_W], mixed[GRID_W:]).astype(BF16)
                )
            attended = jnp.concatenate(attended, axis=1)
            for shift in list(range(1, n_tp)) + [0]:
                block = tp_at(shift)
                w_rows = pl.ds(pl.multiple_of(block * feats, feats), feats)
                product = lax.dot_general(
                    attended, w_full[base + 3, w_rows], (((1,), (1,)), ((), ())),
                    preferred_element_type=F32,
                )
                part[layer, block, q_rows] = product.astype(BF16)
                if shift:
                    r_copy(row, shift).start()
            return 0

        lax.fori_loop(0, rows_dev, attend, 0)

        if layer + 1 < layers:
            for slot in order:
                pass_on(base + 4 + slot)
            expand_layer(layer + 1)
        branch = part[layer, tp].astype(F32)
        for shift in range(1, n_tp):
            for row in range(rows_dev):
                r_copy(row, shift).wait_recv()
            branch = branch + rs_buf[layer, tp_at(n_tp - shift)].astype(F32)
        squares = jnp.sum(branch * branch, axis=1, keepdims=True)
        flat = jnp.transpose(jnp.broadcast_to(squares, (tokens, 128)))
        sq_own[layer] = flat[0:8]

        def s_copy(shift):
            return remote(
                sq_own.at[layer], sq_buf.at[layer, tp],
                s_send.at[layer, shift], s_recv.at[layer, shift], {"tp": tp_at(shift)},
            )

        for shift in range(1, n_tp):
            s_copy(shift).start()
        summed = sq_own[layer]
        for shift in range(1, n_tp):
            s_copy(shift).wait_recv()
            summed = summed + sq_buf[layer, tp_at(n_tp - shift)]
        column = jnp.transpose(jnp.broadcast_to(summed[0:1], (128, tokens)))[:, 0:1]
        out_inverse = lax.rsqrt(column / d_model + EPS)
        before = x_ref[...] if layer == 0 else res[layer - 1]
        after = (
            before.astype(F32) + branch * out_inverse * post_ref[layer:layer + 1, :]
        ).astype(BF16)
        if layer + 1 < layers:
            res[layer] = after
            x_full[layer + 1, tp] = after
            for shift in range(1, n_tp):
                x_copy(layer + 1, shift, res.at[layer]).start()
            for slot in order:
                pass_across(base + 4 + slot)
        else:
            out_ref[...] = after
        for shift in range(1, n_tp):
            x_copy(layer, shift, x_ref).wait_send()
            for row in range(rows_dev):
                r_copy(row, shift).wait_send()
            s_copy(shift).wait_send()
        for which in range(2):
            @pl.when(has_next)
            def _():
                halo_copy(layer, 0, which).wait_send()

            @pl.when(has_prev)
            def _():
                halo_copy(layer, 1, which).wait_send()
        for slot in range(base, base + 4):
            drain_weight(slot)


def shards(
    stream, documents, q_weight, k_weight, v_weight, out_weight, pre_gain, post_gain, offset_bias
):
    n_sp, n_tp, n_grp = lax.axis_size("sp"), lax.axis_size("tp"), lax.axis_size("grp")
    tokens, feats = stream.shape
    layers, rows_w, width = q_weight.shape
    rows_dev = tokens // GRID_W
    n_pair = width // 128
    d_model = feats * n_tp
    n_off = 2 * NA_ROWS - 2
    grid_docs = documents.reshape(rows_dev, 1, GRID_W)
    doc_key = jnp.broadcast_to(
        jnp.concatenate([grid_docs, grid_docs], axis=2), (rows_dev, 8, 2 * GRID_W)
    )
    table = jnp.pad(
        offset_bias.reshape(layers * n_pair * 2, 2 * NA_ROWS - 1, 2 * NA_COLS - 1),
        ((0, 0), (0, 1), (0, 128 - 2 * NA_COLS + 1)),
    )
    n_y = n_sp // 2
    slots = 4 * layers
    ext = tokens + 2 * HALO
    dma = pltpu.SemaphoreType.DMA
    vmem = pl.BlockSpec(memory_space=pltpu.VMEM)
    hbm = pl.BlockSpec(memory_space=pl.ANY)
    return pl.pallas_call(
        functools.partial(kernel, n_sp, n_tp, n_grp, layers, tokens),
        out_shape=jax.ShapeDtypeStruct((tokens, feats), BF16),
        in_specs=[vmem] * 2 + [hbm] * 4 + [vmem] * 3,
        out_specs=vmem,
        scratch_shapes=[
            pltpu.VMEM((slots, d_model, width), BF16),
            pltpu.VMEM((layers, n_tp, tokens, feats), BF16),
            pltpu.VMEM((tokens, d_model), BF16),
            pltpu.VMEM((tokens, width), BF16),
            pltpu.VMEM((layers, ext, width), BF16),
            pltpu.VMEM((layers, ext, width), BF16),
            pltpu.VMEM((rows_dev + 2 * HALF, 8, 128), jnp.int32),
            pltpu.VMEM((layers, n_tp, tokens, feats), BF16),
            pltpu.VMEM((layers, n_tp, tokens, feats), BF16),
            pltpu.VMEM((layers, tokens, feats), BF16),
            pltpu.VMEM((layers, 8, tokens), F32),
            pltpu.VMEM((layers, n_tp, 8, tokens), F32),
            pltpu.VMEM((layers * n_pair, n_off, 128, 128), F32),
            pltpu.VMEM((rows_dev, NA_ROWS // 2, 128, 128), F32),
            dma((slots,)),
            dma((slots, n_y)), dma((slots, n_y)),
            dma((slots,)), dma((slots,)),
            dma((slots, n_y, n_grp)), dma((slots, n_y, n_grp)),
            dma((slots, n_y, n_grp)), dma((slots, n_y, n_grp)),
            dma,
            dma((layers, n_tp)), dma((layers, n_tp)),
            dma, dma((2,)), dma((2,)),
            dma((layers, 2, 2)), dma((layers, 2, 2)),
            dma((layers, rows_dev, n_tp)), dma((layers, rows_dev, n_tp)),
            dma((layers, n_tp)), dma((layers, n_tp)),
        ],
        compiler_params=pltpu.CompilerParams(
            collective_id=0, has_side_effects=True, vmem_limit_bytes=60 * 1024 * 1024
        ),
    )(
        stream, doc_key, q_weight, k_weight, v_weight, out_weight,
        pre_gain, post_gain, table,
    )


def solution(mesh):
    in_specs = (
        P(("grp", "sp"), "tp"),
        P(("grp", "sp")),
        P(None, "sp", "tp"),
        P(None, "sp", "tp"),
        P(None, "sp", "tp"),
        P(None, "sp", "tp"),
        P(),
        P(None, "tp"),
        P(None, "tp", None, None),
    )
    out_specs = P(("grp", "sp"), "tp")
    return jax.shard_map(shards, mesh=mesh, in_specs=in_specs, out_specs=out_specs, check_vma=False)
```

```python
import functools

import jax
import jax.numpy as jnp
from jax import lax
from jax.experimental import pallas as pl
from jax.experimental.pallas import tpu as pltpu
from jax.sharding import PartitionSpec as P

HEAD_DIM = 64
GRID_W = 64
NA_ROWS = 8
NA_COLS = 16
HALF = NA_ROWS // 2
HALO = HALF * GRID_W
EPS = 1e-06
MESH = pl.DeviceIdType.MESH
F32 = jnp.float32
BF16 = jnp.bfloat16


def kernel(
    n_sp, n_tp, n_grp, layers, tokens,
    x_ref, dock_ref, wq_ref, wk_ref, wv_ref, wo_ref, pre_ref, post_ref, tab_ref,
    out_ref,
    w_full, x_full, x_scaled, q_buf, k_ext, v_ext, d_ext, part, rs_buf, res, sq_own, sq_buf,
    bias, dmask,
    wl_sem, wy_send, wy_recv, wm_send, wm_recv, wf_send, wf_recv, wx_send, wx_recv,
    xl_sem, x_send, x_recv, d_local, d_send, d_recv, h_send, h_recv, r_send, r_recv, s_send, s_recv,
):
    weights = (wq_ref, wk_ref, wv_ref, wo_ref)
    sp, tp, grp = lax.axis_index("sp"), lax.axis_index("tp"), lax.axis_index("grp")
    n_y = n_sp // 2
    y, core = sp // 2, sp % 2
    mate = y * 2 + (1 - core)
    feats = x_ref.shape[1]
    width = wq_ref.shape[2]
    rows_w = wq_ref.shape[1]
    rows_dev = tokens // GRID_W
    n_pair = width // 128
    d_model = n_tp * feats

    def tp_at(shift):
        return (tp + shift) % n_tp

    piece = rows_w // n_grp

    def rows_of(owner):
        return pl.ds(pl.multiple_of(owner * rows_w, rows_w), rows_w)

    def piece_of(owner, index):
        return pl.ds(pl.multiple_of(owner * rows_w + index * piece, piece), piece)

    def remote(src, dst, send, recv, target):
        return pltpu.make_async_remote_copy(
            src_ref=src, dst_ref=dst, send_sem=send, recv_sem=recv,
            device_id=target, device_id_type=MESH,
        )

    barrier = pltpu.get_barrier_semaphore()
    for shift in range(1, n_tp):
        pl.semaphore_signal(barrier, inc=1, device_id={"tp": tp_at(shift)}, device_id_type=MESH)
    for shift in range(1, n_sp):
        pl.semaphore_signal(
            barrier, inc=1, device_id={"sp": (sp + shift) % n_sp}, device_id_type=MESH
        )
    for shift in range(1, n_grp):
        pl.semaphore_signal(
            barrier, inc=1, device_id={"grp": (grp + shift) % n_grp}, device_id_type=MESH
        )
    pl.semaphore_wait(barrier, n_tp + n_sp + n_grp - 3)

    def y_copy(slot, shift):
        own = pl.ds(pl.multiple_of(grp * piece, piece), piece)
        return remote(
            weights[slot % 4].at[slot // 4, own], w_full.at[slot, piece_of(sp, grp)],
            wy_send.at[slot, shift], wy_recv.at[slot, shift],
            {"sp": ((y + shift) % n_y) * 2 + core},
        )

    def mate_copy(slot):
        return remote(
            weights[slot % 4].at[slot // 4], w_full.at[slot, rows_of(sp)],
            wm_send.at[slot], wm_recv.at[slot], {"sp": mate},
        )

    def local_copy(slot):
        return pltpu.make_async_copy(
            weights[slot % 4].at[slot // 4], w_full.at[slot, rows_of(sp)], wl_sem.at[slot]
        )

    def arrived(slot, shift, turn):
        owner = ((y - shift + n_y) % n_y) * 2 + core
        return w_full.at[slot, piece_of(owner, (grp - turn + n_grp) % n_grp)]

    def forward_copy(slot, shift, turn):
        block = arrived(slot, shift, turn)
        return remote(
            block, block, wf_send.at[slot, shift, turn], wf_recv.at[slot, shift, turn],
            {"sp": mate},
        )

    def x_link_copy(slot, shift, turn):
        block = arrived(slot, shift, 0)
        return remote(
            block, block, wx_send.at[slot, shift, turn], wx_recv.at[slot, shift, turn],
            {"grp": (grp + turn) % n_grp},
        )

    def start_weight(slot):
        for shift in range(1, n_y):
            y_copy(slot, shift).start()
        mate_copy(slot).start()
        local_copy(slot).start()

    def pass_on(slot):
        for shift in range(1, n_y):
            y_copy(slot, shift).wait_recv()
            for turn in range(1, n_grp):
                x_link_copy(slot, shift, turn).start()
            forward_copy(slot, shift, 0).start()

    def pass_across(slot):
        for shift in range(1, n_y):
            for turn in range(1, n_grp):
                x_link_copy(slot, shift, turn).wait_recv()
                forward_copy(slot, shift, turn).start()

    def finish_weight(slot):
        local_copy(slot).wait()
        mate_copy(slot).wait_recv()
        for shift in range(1, n_y):
            for turn in range(n_grp):
                forward_copy(slot, shift, turn).wait_recv()

    def drain_weight(slot):
        mate_copy(slot).wait_send()
        for shift in range(1, n_y):
            y_copy(slot, shift).wait_send()
            for turn in range(n_grp):
                forward_copy(slot, shift, turn).wait_send()
            for turn in range(1, n_grp):
                x_link_copy(slot, shift, turn).wait_send()

    def x_copy(layer, shift, source):
        return remote(
            source, x_full.at[layer, tp], x_send.at[layer, shift], x_recv.at[layer, shift],
            {"tp": tp_at(shift)},
        )

    def doc_copy(side):
        if side == 0:
            src, dst, target = dock_ref.at[pl.ds(rows_dev - HALF, HALF)], d_ext.at[pl.ds(0, HALF)], sp + 1
        else:
            src, dst, target = dock_ref.at[pl.ds(0, HALF)], d_ext.at[pl.ds(HALF + rows_dev, HALF)], sp - 1
        return remote(src, dst, d_send.at[side], d_recv.at[side], {"sp": target})

    def halo_copy(layer, side, which):
        buf = (k_ext, v_ext)[which]
        if side == 0:
            src, dst, target = tokens, 0, sp + 1
        else:
            src, dst, target = HALO, HALO + tokens, sp - 1
        return remote(
            buf.at[layer, pl.ds(src, HALO)], buf.at[layer, pl.ds(dst, HALO)],
            h_send.at[layer, side, which], h_recv.at[layer, side, which], {"sp": target},
        )

    has_next, has_prev = sp < n_sp - 1, sp > 0

    order = (1, 2, 0, 3)
    for slot in order[:3]:
        start_weight(slot)
    x_local = pltpu.make_async_copy(x_ref, x_full.at[0, tp], xl_sem)
    x_local.start()
    for shift in range(1, n_tp):
        x_copy(0, shift, x_ref).start()
    d_own = pltpu.make_async_copy(dock_ref, d_ext.at[pl.ds(HALF, rows_dev)], d_local)
    d_own.start()

    @pl.when(has_next)
    def _():
        doc_copy(0).start()

    @pl.when(has_prev)
    def _():
        doc_copy(1).start()

    q_ids = lax.broadcasted_iota(jnp.int32, (GRID_W, 128), 0)
    lanes = lax.broadcasted_iota(jnp.int32, (GRID_W, 128), 1)
    key_col = lanes % GRID_W
    first_col = jnp.clip(q_ids - NA_COLS // 2, 0, GRID_W - NA_COLS)
    col_ok = (key_col >= first_col) & (key_col < first_col + NA_COLS)
    low_half = lanes < GRID_W
    n_off = 2 * NA_ROWS - 2

    def expand(step, _):
        group, offset = step // n_off, step % n_off
        for half in range(2):
            first = tab_ref[group * 2 + half, pl.ds(offset, 1)]
            second = tab_ref[group * 2 + half, pl.ds(offset + 1, 1)]
            row = jnp.broadcast_to(first + pltpu.roll(second, GRID_W, 1), (GRID_W, 128))
            skew = pltpu.roll(row, 128 - (NA_COLS - 1), 1, stride=1, stride_axis=0)
            bias[group, offset, half * GRID_W:(half + 1) * GRID_W] = jnp.where(
                col_ok, skew, -jnp.inf
            )
        return 0

    def expand_layer(layer):
        lax.fori_loop(layer * n_pair * n_off, (layer + 1) * n_pair * n_off, expand, 0)

    expand_layer(0)
    pass_on(order[0])

    d_own.wait()

    @pl.when(has_next)
    def _():
        doc_copy(0).wait_send()
        doc_copy(1).wait_recv()

    @pl.when(has_prev)
    def _():
        doc_copy(1).wait_send()
        doc_copy(0).wait_recv()

    first_row = sp * rows_dev

    def window(row):
        start = jnp.clip(first_row + row - HALF, 0, rows_dev * n_sp - NA_ROWS)
        return start - first_row + HALF

    for row in range(rows_dev):
        own_docs = jnp.broadcast_to(dock_ref[row][0:1].astype(F32), (128, 128))
        q_doc = jnp.transpose(own_docs)[0:GRID_W]
        for pair in range(NA_ROWS // 2):
            at = window(row) + 2 * pair
            k_doc = jnp.where(
                low_half,
                jnp.broadcast_to(d_ext[at][0:1], (GRID_W, 128)),
                jnp.broadcast_to(d_ext[at + 1][0:1], (GRID_W, 128)),
            )
            value = jnp.where(k_doc.astype(F32) == q_doc, 0.0, -jnp.inf).astype(F32)
            dmask[row, pair, 0:GRID_W] = value
            dmask[row, pair, GRID_W:2 * GRID_W] = value

    pass_on(order[1])
    start_weight(order[3])
    pass_across(order[0])
    x_local.wait()

    for layer in range(layers):
        base = 4 * layer
        total = jnp.zeros((tokens, 1), F32)
        for shift in range(n_tp):
            if shift:
                x_copy(layer, shift, x_ref).wait_recv()
            block = tp_at(n_tp - shift)
            span = pl.ds(pl.multiple_of(block * feats, feats), feats)
            wide = x_full[layer, block].astype(F32)
            total = total + jnp.sum(wide * wide, axis=1, keepdims=True)
            x_scaled[:, span] = (wide * pre_ref[layer:layer + 1, span]).astype(BF16)
            if layer == 0 and shift == min(1, n_tp - 1):
                pass_on(order[2])
                pass_across(order[1])
        inverse = lax.rsqrt(total / d_model + EPS)

        if layer == 0:
            pass_on(order[3])
            pass_across(order[2])
        for which in order[:3]:
            finish_weight(base + which)
            product = jnp.dot(x_scaled[...], w_full[base + which], preferred_element_type=F32)
            rounded = (product * inverse).astype(BF16)
            if which == 0:
                q_buf[...] = rounded * jnp.asarray(HEAD_DIM ** -0.5, BF16)
            else:
                buf = (k_ext, v_ext)[which - 1]
                buf[layer, HALO:HALO + tokens] = rounded

                @pl.when(has_next)
                def _():
                    halo_copy(layer, 0, which - 1).start()

                @pl.when(has_prev)
                def _():
                    halo_copy(layer, 1, which - 1).start()

        if layer + 1 < layers:
            for slot in order:
                start_weight(base + 4 + slot)
        if layer == 0:
            pass_across(order[3])

        for which in range(2):
            @pl.when(has_next)
            def _():
                halo_copy(layer, 1, which).wait_recv()

            @pl.when(has_prev)
            def _():
                halo_copy(layer, 0, which).wait_recv()

        finish_weight(base + 3)

        def r_copy(row, shift):
            here = pl.ds(pl.multiple_of(row * GRID_W, GRID_W), GRID_W)
            return remote(
                part.at[layer, tp_at(shift), here], rs_buf.at[layer, tp, here],
                r_send.at[layer, row, shift], r_recv.at[layer, row, shift],
                {"tp": tp_at(shift)},
            )

        def attend(row, _):
            begin = window(row)
            q_rows = pl.ds(pl.multiple_of(row * GRID_W, GRID_W), GRID_W)
            keys = pl.ds(pl.multiple_of(begin * GRID_W, GRID_W), NA_ROWS * GRID_W)
            offset = begin - row + NA_ROWS - 1 - HALF
            attended = []
            for pair in range(n_pair):
                cols = slice(pair * 128, (pair + 1) * 128)
                q2 = q_buf[q_rows, cols]
                zero = jnp.zeros_like(q2)
                stacked = jnp.concatenate(
                    [jnp.where(low_half, q2, zero), jnp.where(low_half, zero, q2)], axis=0
                )
                k2 = k_ext[layer, keys, cols]
                scores = lax.dot_general(
                    stacked, k2, (((1,), (1,)), ((), ())), preferred_element_type=F32
                )
                pieces = []
                for at in range(NA_ROWS // 2):
                    pieces.append(
                        scores[:, at * 128:(at + 1) * 128]
                        + bias[layer * n_pair + pair, offset + 2 * at]
                        + dmask[row, at]
                    )
                full = jnp.concatenate(pieces, axis=1)
                top = jnp.max(full, axis=1, keepdims=True)
                grown = jnp.exp(full - top)
                share = 1.0 / jnp.sum(grown, axis=1, keepdims=True)
                probs = (grown * share).astype(BF16)
                mixed = jnp.dot(probs, v_ext[layer, keys, cols], preferred_element_type=F32)
                attended.append(
                    jnp.where(low_half, mixed[:GRID_W], mixed[GRID_W:]).astype(BF16)
                )
            attended = jnp.concatenate(attended, axis=1)
            for shift in list(range(1, n_tp)) + [0]:
                block = tp_at(shift)
                w_rows = pl.ds(pl.multiple_of(block * feats, feats), feats)
                product = lax.dot_general(
                    attended, w_full[base + 3, w_rows], (((1,), (1,)), ((), ())),
                    preferred_element_type=F32,
                )
                part[layer, block, q_rows] = product.astype(BF16)
                if shift:
                    r_copy(row, shift).start()
            return 0

        lax.fori_loop(0, rows_dev, attend, 0)

        if layer + 1 < layers:
            expand_layer(layer + 1)
            for slot in order:
                pass_on(base + 4 + slot)
        branch = part[layer, tp].astype(F32)
        for shift in range(1, n_tp):
            for row in range(rows_dev):
                r_copy(row, shift).wait_recv()
            branch = branch + rs_buf[layer, tp_at(n_tp - shift)].astype(F32)
        squares = jnp.sum(branch * branch, axis=1, keepdims=True)
        flat = jnp.transpose(jnp.broadcast_to(squares, (tokens, 128)))
        sq_own[layer] = flat[0:8]

        def s_copy(shift):
            return remote(
                sq_own.at[layer], sq_buf.at[layer, tp],
                s_send.at[layer, shift], s_recv.at[layer, shift], {"tp": tp_at(shift)},
            )

        for shift in range(1, n_tp):
            s_copy(shift).start()
        summed = sq_own[layer]
        for shift in range(1, n_tp):
            s_copy(shift).wait_recv()
            summed = summed + sq_buf[layer, tp_at(n_tp - shift)]
        column = jnp.transpose(jnp.broadcast_to(summed[0:1], (128, tokens)))[:, 0:1]
        out_inverse = lax.rsqrt(column / d_model + EPS)
        before = x_ref[...] if layer == 0 else res[layer - 1]
        after = (
            before.astype(F32) + branch * out_inverse * post_ref[layer:layer + 1, :]
        ).astype(BF16)
        if layer + 1 < layers:
            res[layer] = after
            x_full[layer + 1, tp] = after
            for shift in range(1, n_tp):
                x_copy(layer + 1, shift, res.at[layer]).start()
            for slot in order:
                pass_across(base + 4 + slot)
        else:
            out_ref[...] = after
        for shift in range(1, n_tp):
            x_copy(layer, shift, x_ref).wait_send()
            for row in range(rows_dev):
                r_copy(row, shift).wait_send()
            s_copy(shift).wait_send()
        for which in range(2):
            @pl.when(has_next)
            def _():
                halo_copy(layer, 0, which).wait_send()

            @pl.when(has_prev)
            def _():
                halo_copy(layer, 1, which).wait_send()
        for slot in range(base, base + 4):
            drain_weight(slot)


def shards(
    stream, documents, q_weight, k_weight, v_weight, out_weight, pre_gain, post_gain, offset_bias
):
    n_sp, n_tp, n_grp = lax.axis_size("sp"), lax.axis_size("tp"), lax.axis_size("grp")
    tokens, feats = stream.shape
    layers, rows_w, width = q_weight.shape
    rows_dev = tokens // GRID_W
    n_pair = width // 128
    d_model = feats * n_tp
    n_off = 2 * NA_ROWS - 2
    grid_docs = documents.reshape(rows_dev, 1, GRID_W)
    doc_key = jnp.broadcast_to(
        jnp.concatenate([grid_docs, grid_docs], axis=2), (rows_dev, 8, 2 * GRID_W)
    )
    table = jnp.pad(
        offset_bias.reshape(layers * n_pair * 2, 2 * NA_ROWS - 1, 2 * NA_COLS - 1),
        ((0, 0), (0, 1), (0, 128 - 2 * NA_COLS + 1)),
    )
    n_y = n_sp // 2
    slots = 4 * layers
    ext = tokens + 2 * HALO
    dma = pltpu.SemaphoreType.DMA
    vmem = pl.BlockSpec(memory_space=pltpu.VMEM)
    hbm = pl.BlockSpec(memory_space=pl.ANY)
    return pl.pallas_call(
        functools.partial(kernel, n_sp, n_tp, n_grp, layers, tokens),
        out_shape=jax.ShapeDtypeStruct((tokens, feats), BF16),
        in_specs=[vmem] * 2 + [hbm] * 4 + [vmem] * 3,
        out_specs=vmem,
        scratch_shapes=[
            pltpu.VMEM((slots, d_model, width), BF16),
            pltpu.VMEM((layers, n_tp, tokens, feats), BF16),
            pltpu.VMEM((tokens, d_model), BF16),
            pltpu.VMEM((tokens, width), BF16),
            pltpu.VMEM((layers, ext, width), BF16),
            pltpu.VMEM((layers, ext, width), BF16),
            pltpu.VMEM((rows_dev + 2 * HALF, 8, 128), jnp.int32),
            pltpu.VMEM((layers, n_tp, tokens, feats), BF16),
            pltpu.VMEM((layers, n_tp, tokens, feats), BF16),
            pltpu.VMEM((layers, tokens, feats), BF16),
            pltpu.VMEM((layers, 8, tokens), F32),
            pltpu.VMEM((layers, n_tp, 8, tokens), F32),
            pltpu.VMEM((layers * n_pair, n_off, 128, 128), F32),
            pltpu.VMEM((rows_dev, NA_ROWS // 2, 128, 128), F32),
            dma((slots,)),
            dma((slots, n_y)), dma((slots, n_y)),
            dma((slots,)), dma((slots,)),
            dma((slots, n_y, n_grp)), dma((slots, n_y, n_grp)),
            dma((slots, n_y, n_grp)), dma((slots, n_y, n_grp)),
            dma,
            dma((layers, n_tp)), dma((layers, n_tp)),
            dma, dma((2,)), dma((2,)),
            dma((layers, 2, 2)), dma((layers, 2, 2)),
            dma((layers, rows_dev, n_tp)), dma((layers, rows_dev, n_tp)),
            dma((layers, n_tp)), dma((layers, n_tp)),
        ],
        compiler_params=pltpu.CompilerParams(
            collective_id=0, has_side_effects=True, vmem_limit_bytes=60 * 1024 * 1024
        ),
    )(
        stream, doc_key, q_weight, k_weight, v_weight, out_weight,
        pre_gain, post_gain, table,
    )


def solution(mesh):
    in_specs = (
        P(("grp", "sp"), "tp"),
        P(("grp", "sp")),
        P(None, "sp", "tp"),
        P(None, "sp", "tp"),
        P(None, "sp", "tp"),
        P(None, "sp", "tp"),
        P(),
        P(None, "tp"),
        P(None, "tp", None, None),
    )
    out_specs = P(("grp", "sp"), "tp")
    return jax.shard_map(shards, mesh=mesh, in_specs=in_specs, out_specs=out_specs, check_vma=False)
```

```python
import functools

import jax
import jax.numpy as jnp
from jax import lax
from jax.experimental import pallas as pl
from jax.experimental.pallas import tpu as pltpu
from jax.sharding import PartitionSpec as P

HEAD_DIM = 64
GRID_W = 64
NA_ROWS = 8
NA_COLS = 16
HALF = NA_ROWS // 2
HALO = HALF * GRID_W
EPS = 1e-06
MESH = pl.DeviceIdType.MESH
F32 = jnp.float32
BF16 = jnp.bfloat16


def kernel(
    n_sp, n_tp, n_grp, layers, tokens,
    x_ref, dock_ref, wq_ref, wk_ref, wv_ref, wo_ref, pre_ref, post_ref, tab_ref,
    out_ref,
    w_full, x_full, x_scaled, q_buf, k_ext, v_ext, d_ext, part, rs_buf, res, sq_own, sq_buf,
    bias, dmask,
    wl_sem, wy_send, wy_recv, wm_send, wm_recv, wf_send, wf_recv, wx_send, wx_recv,
    xl_sem, x_send, x_recv, d_local, d_send, d_recv, h_send, h_recv, r_send, r_recv, s_send, s_recv,
):
    weights = (wq_ref, wk_ref, wv_ref, wo_ref)
    sp, tp, grp = lax.axis_index("sp"), lax.axis_index("tp"), lax.axis_index("grp")
    n_y = n_sp // 2
    y, core = sp // 2, sp % 2
    mate = y * 2 + (1 - core)
    feats = x_ref.shape[1]
    width = wq_ref.shape[2]
    rows_w = wq_ref.shape[1]
    rows_dev = tokens // GRID_W
    n_pair = width // 128
    d_model = n_tp * feats

    def tp_at(shift):
        return (tp + shift) % n_tp

    piece = rows_w // n_grp

    def rows_of(owner):
        return pl.ds(pl.multiple_of(owner * rows_w, rows_w), rows_w)

    def piece_of(owner, index):
        return pl.ds(pl.multiple_of(owner * rows_w + index * piece, piece), piece)

    def remote(src, dst, send, recv, target):
        return pltpu.make_async_remote_copy(
            src_ref=src, dst_ref=dst, send_sem=send, recv_sem=recv,
            device_id=target, device_id_type=MESH,
        )

    barrier = pltpu.get_barrier_semaphore()
    for shift in range(1, n_tp):
        pl.semaphore_signal(barrier, inc=1, device_id={"tp": tp_at(shift)}, device_id_type=MESH)
    for shift in range(1, n_sp):
        pl.semaphore_signal(
            barrier, inc=1, device_id={"sp": (sp + shift) % n_sp}, device_id_type=MESH
        )
    for shift in range(1, n_grp):
        pl.semaphore_signal(
            barrier, inc=1, device_id={"grp": (grp + shift) % n_grp}, device_id_type=MESH
        )
    pl.semaphore_wait(barrier, n_tp + n_sp + n_grp - 3)

    def y_copy(slot, shift):
        own = pl.ds(pl.multiple_of(grp * piece, piece), piece)
        return remote(
            weights[slot % 4].at[slot // 4, own], w_full.at[slot, piece_of(sp, grp)],
            wy_send.at[slot, shift], wy_recv.at[slot, shift],
            {"sp": ((y + shift) % n_y) * 2 + core},
        )

    def mate_copy(slot):
        return remote(
            weights[slot % 4].at[slot // 4], w_full.at[slot, rows_of(sp)],
            wm_send.at[slot], wm_recv.at[slot], {"sp": mate},
        )

    def local_copy(slot):
        return pltpu.make_async_copy(
            weights[slot % 4].at[slot // 4], w_full.at[slot, rows_of(sp)], wl_sem.at[slot]
        )

    def arrived(slot, shift, turn):
        owner = ((y - shift + n_y) % n_y) * 2 + core
        return w_full.at[slot, piece_of(owner, (grp - turn + n_grp) % n_grp)]

    def forward_copy(slot, shift, turn):
        block = arrived(slot, shift, turn)
        return remote(
            block, block, wf_send.at[slot, shift, turn], wf_recv.at[slot, shift, turn],
            {"sp": mate},
        )

    def x_link_copy(slot, shift, turn):
        block = arrived(slot, shift, 0)
        return remote(
            block, block, wx_send.at[slot, shift, turn], wx_recv.at[slot, shift, turn],
            {"grp": (grp + turn) % n_grp},
        )

    def start_weight(slot):
        for shift in range(1, n_y):
            y_copy(slot, shift).start()
        mate_copy(slot).start()
        local_copy(slot).start()

    def pass_on(slot):
        for shift in range(1, n_y):
            y_copy(slot, shift).wait_recv()
            for turn in range(1, n_grp):
                x_link_copy(slot, shift, turn).start()
            forward_copy(slot, shift, 0).start()

    def pass_across(slot):
        for shift in range(1, n_y):
            for turn in range(1, n_grp):
                x_link_copy(slot, shift, turn).wait_recv()
                forward_copy(slot, shift, turn).start()

    def finish_weight(slot):
        local_copy(slot).wait()
        mate_copy(slot).wait_recv()
        for shift in range(1, n_y):
            for turn in range(n_grp):
                forward_copy(slot, shift, turn).wait_recv()

    def drain_weight(slot):
        mate_copy(slot).wait_send()
        for shift in range(1, n_y):
            y_copy(slot, shift).wait_send()
            for turn in range(n_grp):
                forward_copy(slot, shift, turn).wait_send()
            for turn in range(1, n_grp):
                x_link_copy(slot, shift, turn).wait_send()

    def x_copy(layer, shift, source):
        return remote(
            source, x_full.at[layer, tp], x_send.at[layer, shift], x_recv.at[layer, shift],
            {"tp": tp_at(shift)},
        )

    def doc_copy(side):
        if side == 0:
            src, dst, target = dock_ref.at[pl.ds(rows_dev - HALF, HALF)], d_ext.at[pl.ds(0, HALF)], sp + 1
        else:
            src, dst, target = dock_ref.at[pl.ds(0, HALF)], d_ext.at[pl.ds(HALF + rows_dev, HALF)], sp - 1
        return remote(src, dst, d_send.at[side], d_recv.at[side], {"sp": target})

    def halo_copy(layer, side, which):
        buf = (k_ext, v_ext)[which]
        if side == 0:
            src, dst, target = tokens, 0, sp + 1
        else:
            src, dst, target = HALO, HALO + tokens, sp - 1
        return remote(
            buf.at[layer, pl.ds(src, HALO)], buf.at[layer, pl.ds(dst, HALO)],
            h_send.at[layer, side, which], h_recv.at[layer, side, which], {"sp": target},
        )

    has_next, has_prev = sp < n_sp - 1, sp > 0

    order = (1, 2, 0, 3)
    for slot in order[:3]:
        start_weight(slot)
    x_local = pltpu.make_async_copy(x_ref, x_full.at[0, tp], xl_sem)
    x_local.start()
    for shift in range(1, n_tp):
        x_copy(0, shift, x_ref).start()
    d_own = pltpu.make_async_copy(dock_ref, d_ext.at[pl.ds(HALF, rows_dev)], d_local)
    d_own.start()

    @pl.when(has_next)
    def _():
        doc_copy(0).start()

    @pl.when(has_prev)
    def _():
        doc_copy(1).start()

    q_ids = lax.broadcasted_iota(jnp.int32, (GRID_W, 128), 0)
    lanes = lax.broadcasted_iota(jnp.int32, (GRID_W, 128), 1)
    key_col = lanes % GRID_W
    first_col = jnp.clip(q_ids - NA_COLS // 2, 0, GRID_W - NA_COLS)
    col_ok = (key_col >= first_col) & (key_col < first_col + NA_COLS)
    low_half = lanes < GRID_W
    n_off = 2 * NA_ROWS - 2

    def expand(step, _):
        group, offset = step // n_off, step % n_off
        for half in range(2):
            first = tab_ref[group * 2 + half, pl.ds(offset, 1)]
            second = tab_ref[group * 2 + half, pl.ds(offset + 1, 1)]
            row = jnp.broadcast_to(first + pltpu.roll(second, GRID_W, 1), (GRID_W, 128))
            skew = pltpu.roll(row, 128 - (NA_COLS - 1), 1, stride=1, stride_axis=0)
            bias[group, offset, half * GRID_W:(half + 1) * GRID_W] = jnp.where(
                col_ok, skew, -jnp.inf
            )
        return 0

    def expand_layer(layer):
        lax.fori_loop(layer * n_pair * n_off, (layer + 1) * n_pair * n_off, expand, 0)

    expand_layer(0)
    pass_on(order[0])

    d_own.wait()

    @pl.when(has_next)
    def _():
        doc_copy(0).wait_send()
        doc_copy(1).wait_recv()

    @pl.when(has_prev)
    def _():
        doc_copy(1).wait_send()
        doc_copy(0).wait_recv()

    first_row = sp * rows_dev

    def window(row):
        start = jnp.clip(first_row + row - HALF, 0, rows_dev * n_sp - NA_ROWS)
        return start - first_row + HALF

    for row in range(rows_dev):
        own_docs = jnp.broadcast_to(dock_ref[row][0:1].astype(F32), (128, 128))
        q_doc = jnp.transpose(own_docs)[0:GRID_W]
        for pair in range(NA_ROWS // 2):
            at = window(row) + 2 * pair
            k_doc = jnp.where(
                low_half,
                jnp.broadcast_to(d_ext[at][0:1], (GRID_W, 128)),
                jnp.broadcast_to(d_ext[at + 1][0:1], (GRID_W, 128)),
            )
            value = jnp.where(k_doc.astype(F32) == q_doc, 0.0, -jnp.inf).astype(F32)
            dmask[row, pair, 0:GRID_W] = value
            dmask[row, pair, GRID_W:2 * GRID_W] = value

    pass_on(order[1])
    start_weight(order[3])
    pass_across(order[0])
    x_local.wait()

    for layer in range(layers):
        base = 4 * layer
        total = jnp.zeros((tokens, 1), F32)
        for shift in range(n_tp):
            if shift:
                x_copy(layer, shift, x_ref).wait_recv()
            block = tp_at(n_tp - shift)
            span = pl.ds(pl.multiple_of(block * feats, feats), feats)
            wide = x_full[layer, block].astype(F32)
            total = total + jnp.sum(wide * wide, axis=1, keepdims=True)
            x_scaled[:, span] = (wide * pre_ref[layer:layer + 1, span]).astype(BF16)
            if layer == 0 and shift == min(1, n_tp - 1):
                pass_on(order[2])
                pass_across(order[1])
        inverse = lax.rsqrt(total / d_model + EPS)

        if layer == 0:
            pass_on(order[3])
            pass_across(order[2])
        for which in order[:3]:
            finish_weight(base + which)
            product = jnp.dot(x_scaled[...], w_full[base + which], preferred_element_type=F32)
            rounded = (product * inverse).astype(BF16)
            if which == 0:
                q_buf[...] = rounded * jnp.asarray(HEAD_DIM ** -0.5, BF16)
            else:
                buf = (k_ext, v_ext)[which - 1]
                buf[layer, HALO:HALO + tokens] = rounded

                @pl.when(has_next)
                def _():
                    halo_copy(layer, 0, which - 1).start()

                @pl.when(has_prev)
                def _():
                    halo_copy(layer, 1, which - 1).start()

        if layer + 1 < layers:
            for slot in order:
                start_weight(base + 4 + slot)

        for which in range(2):
            @pl.when(has_next)
            def _():
                halo_copy(layer, 1, which).wait_recv()

            @pl.when(has_prev)
            def _():
                halo_copy(layer, 0, which).wait_recv()

        def r_copy(row, shift):
            here = pl.ds(pl.multiple_of(row * GRID_W, GRID_W), GRID_W)
            return remote(
                part.at[layer, tp_at(shift), here], rs_buf.at[layer, tp, here],
                r_send.at[layer, row, shift], r_recv.at[layer, row, shift],
                {"tp": tp_at(shift)},
            )

        def attend(row, _):
            begin = window(row)
            q_rows = pl.ds(pl.multiple_of(row * GRID_W, GRID_W), GRID_W)
            keys = pl.ds(pl.multiple_of(begin * GRID_W, GRID_W), NA_ROWS * GRID_W)
            offset = begin - row + NA_ROWS - 1 - HALF
            attended = []
            for pair in range(n_pair):
                cols = slice(pair * 128, (pair + 1) * 128)
                q2 = q_buf[q_rows, cols]
                zero = jnp.zeros_like(q2)
                stacked = jnp.concatenate(
                    [jnp.where(low_half, q2, zero), jnp.where(low_half, zero, q2)], axis=0
                )
                k2 = k_ext[layer, keys, cols]
                scores = lax.dot_general(
                    stacked, k2, (((1,), (1,)), ((), ())), preferred_element_type=F32
                )
                pieces = []
                for at in range(NA_ROWS // 2):
                    pieces.append(
                        scores[:, at * 128:(at + 1) * 128]
                        + bias[layer * n_pair + pair, offset + 2 * at]
                        + dmask[row, at]
                    )
                full = jnp.concatenate(pieces, axis=1)
                top = jnp.max(full, axis=1, keepdims=True)
                grown = jnp.exp(full - top)
                share = 1.0 / jnp.sum(grown, axis=1, keepdims=True)
                probs = (grown * share).astype(BF16)
                mixed = jnp.dot(probs, v_ext[layer, keys, cols], preferred_element_type=F32)
                attended.append(
                    jnp.where(low_half, mixed[:GRID_W], mixed[GRID_W:]).astype(BF16)
                )
            attended = jnp.concatenate(attended, axis=1)

            @pl.when(row == 0)
            def _():
                if layer == 0:
                    pass_across(order[3])
                finish_weight(base + 3)

            for shift in list(range(1, n_tp)) + [0]:
                block = tp_at(shift)
                w_rows = pl.ds(pl.multiple_of(block * feats, feats), feats)
                product = lax.dot_general(
                    attended, w_full[base + 3, w_rows], (((1,), (1,)), ((), ())),
                    preferred_element_type=F32,
                )
                part[layer, block, q_rows] = product.astype(BF16)
                if shift:
                    r_copy(row, shift).start()
            return 0

        lax.fori_loop(0, rows_dev, attend, 0)

        if layer + 1 < layers:
            expand_layer(layer + 1)
            for slot in order:
                pass_on(base + 4 + slot)
        branch = part[layer, tp].astype(F32)
        for shift in range(1, n_tp):
            for row in range(rows_dev):
                r_copy(row, shift).wait_recv()
            branch = branch + rs_buf[layer, tp_at(n_tp - shift)].astype(F32)
        squares = jnp.sum(branch * branch, axis=1, keepdims=True)
        flat = jnp.transpose(jnp.broadcast_to(squares, (tokens, 128)))
        sq_own[layer] = flat[0:8]

        def s_copy(shift):
            return remote(
                sq_own.at[layer], sq_buf.at[layer, tp],
                s_send.at[layer, shift], s_recv.at[layer, shift], {"tp": tp_at(shift)},
            )

        for shift in range(1, n_tp):
            s_copy(shift).start()
        summed = sq_own[layer]
        for shift in range(1, n_tp):
            s_copy(shift).wait_recv()
            summed = summed + sq_buf[layer, tp_at(n_tp - shift)]
        column = jnp.transpose(jnp.broadcast_to(summed[0:1], (128, tokens)))[:, 0:1]
        out_inverse = lax.rsqrt(column / d_model + EPS)
        before = x_ref[...] if layer == 0 else res[layer - 1]
        after = (
            before.astype(F32) + branch * out_inverse * post_ref[layer:layer + 1, :]
        ).astype(BF16)
        if layer + 1 < layers:
            res[layer] = after
            x_full[layer + 1, tp] = after
            for shift in range(1, n_tp):
                x_copy(layer + 1, shift, res.at[layer]).start()
            for slot in order:
                pass_across(base + 4 + slot)
        else:
            out_ref[...] = after
        for shift in range(1, n_tp):
            x_copy(layer, shift, x_ref).wait_send()
            for row in range(rows_dev):
                r_copy(row, shift).wait_send()
            s_copy(shift).wait_send()
        for which in range(2):
            @pl.when(has_next)
            def _():
                halo_copy(layer, 0, which).wait_send()

            @pl.when(has_prev)
            def _():
                halo_copy(layer, 1, which).wait_send()
        for slot in range(base, base + 4):
            drain_weight(slot)


def shards(
    stream, documents, q_weight, k_weight, v_weight, out_weight, pre_gain, post_gain, offset_bias
):
    n_sp, n_tp, n_grp = lax.axis_size("sp"), lax.axis_size("tp"), lax.axis_size("grp")
    tokens, feats = stream.shape
    layers, rows_w, width = q_weight.shape
    rows_dev = tokens // GRID_W
    n_pair = width // 128
    d_model = feats * n_tp
    n_off = 2 * NA_ROWS - 2
    grid_docs = documents.reshape(rows_dev, 1, GRID_W)
    doc_key = jnp.broadcast_to(
        jnp.concatenate([grid_docs, grid_docs], axis=2), (rows_dev, 8, 2 * GRID_W)
    )
    table = jnp.pad(
        offset_bias.reshape(layers * n_pair * 2, 2 * NA_ROWS - 1, 2 * NA_COLS - 1),
        ((0, 0), (0, 1), (0, 128 - 2 * NA_COLS + 1)),
    )
    n_y = n_sp // 2
    slots = 4 * layers
    ext = tokens + 2 * HALO
    dma = pltpu.SemaphoreType.DMA
    vmem = pl.BlockSpec(memory_space=pltpu.VMEM)
    hbm = pl.BlockSpec(memory_space=pl.ANY)
    return pl.pallas_call(
        functools.partial(kernel, n_sp, n_tp, n_grp, layers, tokens),
        out_shape=jax.ShapeDtypeStruct((tokens, feats), BF16),
        in_specs=[vmem] * 2 + [hbm] * 4 + [vmem] * 3,
        out_specs=vmem,
        scratch_shapes=[
            pltpu.VMEM((slots, d_model, width), BF16),
            pltpu.VMEM((layers, n_tp, tokens, feats), BF16),
            pltpu.VMEM((tokens, d_model), BF16),
            pltpu.VMEM((tokens, width), BF16),
            pltpu.VMEM((layers, ext, width), BF16),
            pltpu.VMEM((layers, ext, width), BF16),
            pltpu.VMEM((rows_dev + 2 * HALF, 8, 128), jnp.int32),
            pltpu.VMEM((layers, n_tp, tokens, feats), BF16),
            pltpu.VMEM((layers, n_tp, tokens, feats), BF16),
            pltpu.VMEM((layers, tokens, feats), BF16),
            pltpu.VMEM((layers, 8, tokens), F32),
            pltpu.VMEM((layers, n_tp, 8, tokens), F32),
            pltpu.VMEM((layers * n_pair, n_off, 128, 128), F32),
            pltpu.VMEM((rows_dev, NA_ROWS // 2, 128, 128), F32),
            dma((slots,)),
            dma((slots, n_y)), dma((slots, n_y)),
            dma((slots,)), dma((slots,)),
            dma((slots, n_y, n_grp)), dma((slots, n_y, n_grp)),
            dma((slots, n_y, n_grp)), dma((slots, n_y, n_grp)),
            dma,
            dma((layers, n_tp)), dma((layers, n_tp)),
            dma, dma((2,)), dma((2,)),
            dma((layers, 2, 2)), dma((layers, 2, 2)),
            dma((layers, rows_dev, n_tp)), dma((layers, rows_dev, n_tp)),
            dma((layers, n_tp)), dma((layers, n_tp)),
        ],
        compiler_params=pltpu.CompilerParams(
            collective_id=0, has_side_effects=True, vmem_limit_bytes=60 * 1024 * 1024
        ),
    )(
        stream, doc_key, q_weight, k_weight, v_weight, out_weight,
        pre_gain, post_gain, table,
    )


def solution(mesh):
    in_specs = (
        P(("grp", "sp"), "tp"),
        P(("grp", "sp")),
        P(None, "sp", "tp"),
        P(None, "sp", "tp"),
        P(None, "sp", "tp"),
        P(None, "sp", "tp"),
        P(),
        P(None, "tp"),
        P(None, "tp", None, None),
    )
    out_specs = P(("grp", "sp"), "tp")
    return jax.shard_map(shards, mesh=mesh, in_specs=in_specs, out_specs=out_specs, check_vma=False)
```
